128 devices in a mesh: ep: 16 (over z, x), tp: 8 (over y, core).
Axes of the slice: x: 4, y: 4, z: 4, core: 2. Of those that a mesh axis runs over, the one named last changes fastest.
Arguments:
- tokens: bfloat16 [512, 2048], P('ep'), may hold values from -6 to 6
- lengths: int32 [512], P('ep'), may hold values from 128 to 1024, as said below
- cache_keys: bfloat16 [512, 1024, 1024], P('ep', None, 'tp'), may hold values from -140 to 140
- cache_values: bfloat16 [512, 1024, 1024], P('ep', None, 'tp'), may hold values from -6 to 6
- attn_gain: float32 [2048], replicated, may hold values from 0.1 to 1.9
- q_first_w: bfloat16 [2048, 512], P(None, 'tp'), may hold values from -0.19921875 to 0.19921875
- q_second_w: bfloat16 [2048, 512], P(None, 'tp'), may hold values from -0.19921875 to 0.19921875
- k_first_w: bfloat16 [2048, 512], P(None, 'tp'), may hold values from -0.125 to 0.125
- k_second_w: bfloat16 [2048, 512], P(None, 'tp'), may hold values from -0.125 to 0.125
- value_w: bfloat16 [2048, 1024], P(None, 'tp'), may hold values from -0.125 to 0.125
- mix_lambda: float32 [8], P('tp'), may hold values from 0.3 to 0.8
- head_gain: float32 [128], replicated, may hold values from 0.1 to 1.9
- out_w: bfloat16 [1024, 2048], P('tp'), may hold values from -0.09375 to 0.09375
- ffn_gain: float32 [2048], replicated, may hold values from 0.1 to 1.9
- routes: int32 [512, 4], P('ep'), may hold values from 0 to 63, all different within a row; in each aligned block of 32 rows (0 to 31, 32 to 63, ...) at most 4 rows name the same one
- route_logits: float32 [512, 4], P('ep'), may hold values from -4 to 4
- gate_w: bfloat16 [64, 2048, 1024], P('ep', None, 'tp'), may hold values from -0.34960938 to 0.34960938
- up_w: bfloat16 [64, 2048, 1024], P('ep', None, 'tp'), may hold values from -0.34960938 to 0.34960938
- down_w: bfloat16 [64, 1024, 2048], P('ep', None, 'tp'), may hold values from -0.125 to 0.125
Outputs:
- mixed: bfloat16 [512, 2048], P('ep', 'tp')
The draws below stay inside these ranges and needn't reach their ends.
Inputs may be any that keep to these rules, and one draw needn't show every extreme that they name: `lengths`: at least 128 positions; among the 32 sequences of each index of ep one holds exactly 1024. `routes`: each row names 4 different experts; within the rows of one device no expert is named more than 4 times, a bound that some block reaches.
All inputs are finite; a program needn't handle non-finite values.
Results may differ from the reference program's by a relative error of at most 0.015.
Values may be sent and summed in bfloat16 or wider, within the bound.
A program may use at most 128 MiB of HBM per device.

```python
import math
import jax
import jax.numpy as jnp
import numpy as np
from jax import lax

D = 2048
HEADS = 8
HEAD_DIM = 128
HALF = 64
FF = 1024
EXPERTS = 64
TOP = 4
SEQ_GRP = 32
CACHE = 1024
SEQS = 512
CAP = 4
N_EP = 16


def draw_tokens(key, part):
    column = jnp.arange(D, dtype=jnp.float32) / max(D - 1, 1)
    col_scale = jnp.exp(jnp.log(0.2) + jnp.log(10.0) * column)[None, :]
    noise = jnp.clip(jax.random.normal(key, (SEQS, D), jnp.float32), -3.0, 3.0)
    return (noise * col_scale).astype(jnp.bfloat16)


def draw_lengths(key, part):
    lowest = max(4, CACHE // 8)
    spread = jax.random.randint(key, (SEQS,), lowest, CACHE + 1)
    groups = SEQS // SEQ_GRP
    picks = jax.random.randint(jax.random.fold_in(key, 7), (groups,), 0, SEQ_GRP)
    places = jnp.arange(SEQS, dtype=jnp.int32)
    longest = places % SEQ_GRP == jnp.repeat(picks, SEQ_GRP)
    return jnp.where(longest, CACHE, spread).astype(jnp.int32)


def draw_cache_keys(key, part):
    width = HEADS * HEAD_DIM
    noise = jnp.clip(jax.random.normal(key, (SEQS, CACHE, width), jnp.float32), -5.0, 5.0)
    return noise.astype(jnp.bfloat16)


def block_levels(key, dims, pieces, least, top_value):
    loudness = 1.0
    for dim, shards_of in pieces:
        draws = jax.random.uniform(jax.random.fold_in(jax.random.fold_in(key, 6), dim), (shards_of,), jnp.float32, least / len(pieces), top_value / len(pieces))
        loudness = loudness * jnp.repeat(jnp.exp(draws), dims[dim] // shards_of).reshape((-1,) + (1,) * (len(dims) - 1 - dim))
    return loudness


def deal_out(stream_key, own, number, rows, amount, top, most, lean):
    order = jax.random.permutation(stream_key, amount)
    heavy_load, usual = load_shares(amount, rows * top, most, lean, True), load_shares(amount, rows * top, most, lean, False)
    places = jnp.arange(amount)

    def named(sizes, turn):
        used = int((sizes > 0).sum())
        fixed = max(1, used // 4)
        moved = fixed + (places - fixed + turn * (used - fixed)) % max(1, amount - fixed)
        return jnp.zeros((amount,), jnp.int32).at[order[jnp.where(places < fixed, places, moved)]].set(jnp.asarray(sizes, jnp.int32))

    sizes = jnp.where(number % 4 == 0, named(heavy_load, number // 4), named(usual, number - number // 4 - 1))
    mixed = jax.random.permutation(jax.random.fold_in(own, 3), amount)
    source_of, sink = mixed[0:amount // 2 * 2:2], mixed[1:amount // 2 * 2:2]
    room = jnp.minimum(sizes[source_of] - 1, most - sizes[sink]) // 2
    room = jnp.where((source_of == order[0]) | (sink == order[0]) | (sizes[sink] == 0), 0, jnp.maximum(room, 0))
    moved = jax.random.randint(jax.random.fold_in(own, 4), (amount // 2,), 0, 1 << 20) % (room + 1)
    sizes = sizes.at[source_of].add(-moved).at[sink].add(moved)
    members = jnp.searchsorted(jnp.cumsum(sizes), jnp.arange(rows * top), side="right").astype(jnp.int32)
    grid = members.reshape(top, rows).T
    grid = grid[jax.random.permutation(jax.random.fold_in(own, 1), rows)]
    turn = jax.random.randint(jax.random.fold_in(own, 2), (rows, 1), 0, top)
    return jnp.take_along_axis(grid, (jnp.arange(top)[None, :] + turn) % top, axis=1)


def load_shares(amount, total, limit, lean, full):
    loads = [(1 << 20) // math.isqrt(grade ** lean) + 1 for grade in range(1, amount + 1)]
    largest = limit if full else min(limit, max(-(-total // amount), total * loads[0] // sum(loads)))
    least = 1 if total - largest >= amount - 1 else 0
    given, surplus = [largest] + [least] * (amount - 1), total - largest - least * (amount - 1)
    while surplus > 0:
        free = [i for i in range(1, amount) if given[i] < largest] or [i for i in range(1, amount) if given[i] < limit]
        pool, budget = sum([loads[i] for i in free]), surplus
        for i in free:
            addition = min(limit - given[i], max(1, budget * loads[i] // pool), surplus)
            given[i] = given[i] + addition
            surplus = surplus - addition
    return np.array(given)


def bell_draw(rng, extent, scale, limit, pieces=(), held_as=jnp.bfloat16):
    factor_of = block_levels(rng, extent, pieces, -0.22, 0.18) if pieces else 1.0
    result = jax.random.normal(rng, extent, jnp.float32) * scale * factor_of
    return jnp.minimum(jnp.maximum(result, -limit), limit).astype(held_as)


def setup_inputs(seed: int = 0) -> dict:
    key_list = jax.random.split(jax.random.key(seed), 20)
    tokens = draw_tokens(jax.random.fold_in(key_list[19], 71), 0)
    lengths = draw_lengths(jax.random.fold_in(key_list[19], 71), 0)
    cache_keys = draw_cache_keys(jax.random.fold_in(key_list[19], 71), 0)
    cache_values = bell_draw(key_list[3], (SEQS, CACHE, HEADS * HEAD_DIM), 1.0, 6.0, ((0, 16), (2, 8)))
    attn_gain = jnp.clip(1.0 + 0.18 * jax.random.normal(key_list[4], (D,), jnp.float32), 0.1, 1.9)
    q_first_w = bell_draw(key_list[5], (D, HEADS * HALF), 0.0387, 0.19921875, ((1, 8),))
    q_second_w = bell_draw(key_list[6], (D, HEADS * HALF), 0.0387, 0.19921875, ((1, 8),))
    k_first_w = bell_draw(key_list[7], (D, HEADS * HALF), D ** -0.5, 0.125, ((1, 8),))
    k_second_w = bell_draw(key_list[8], (D, HEADS * HALF), D ** -0.5, 0.125, ((1, 8),))
    value_w = bell_draw(key_list[9], (D, HEADS * HEAD_DIM), D ** -0.5, 0.125, ((1, 8),))
    mix_lambda = jnp.clip(0.3 + 0.5 * jax.random.uniform(key_list[10], (HEADS,), jnp.float32) ** block_levels(key_list[10], (HEADS,), ((0, 8),), -0.2, 0.2), 0.3, 0.8)
    head_gain = jnp.clip(1.0 + 0.18 * jax.random.normal(key_list[11], (HEAD_DIM,), jnp.float32), 0.1, 1.9)
    out_w = bell_draw(key_list[12], (HEADS * HEAD_DIM, D), (0.5 * (HEADS * HEAD_DIM) ** -0.5), 0.09375, ((0, 8),))
    ffn_gain = jnp.clip(1.0 + 0.18 * jax.random.normal(key_list[13], (D,), jnp.float32), 0.1, 1.9)
    routes_keys = jax.random.split(jax.random.fold_in(key_list[14], 1), SEQS // SEQ_GRP)
    routes_turns = jax.random.permutation(jax.random.fold_in(key_list[14], 3), SEQS // SEQ_GRP)
    routes = jax.vmap(lambda own, number: deal_out(jax.random.fold_in(key_list[14], 2), own, number, SEQ_GRP, EXPERTS, TOP, CAP, 2))(routes_keys, routes_turns).reshape((SEQS, TOP))
    route_logits = bell_draw(key_list[15], (SEQS, TOP), 1.0, 4.0, ((0, 16),), jnp.float32)
    gate_w = bell_draw(key_list[16], (EXPERTS, D, FF), 0.066, 0.34960938, ((0, 16), (2, 8)))
    up_w = bell_draw(key_list[17], (EXPERTS, D, FF), 0.066, 0.34960938, ((0, 16), (2, 8)))
    down_w = bell_draw(key_list[18], (EXPERTS, FF, D), (2 * FF) ** -0.5, 0.125, ((0, 16), (2, 8)))
    return {"tokens": tokens, "lengths": lengths, "cache_keys": cache_keys, "cache_values": cache_values, "attn_gain": attn_gain, "q_first_w": q_first_w, "q_second_w": q_second_w, "k_first_w": k_first_w, "k_second_w": k_second_w, "value_w": value_w, "mix_lambda": mix_lambda, "head_gain": head_gain, "out_w": out_w, "ffn_gain": ffn_gain, "routes": routes, "route_logits": route_logits, "gate_w": gate_w, "up_w": up_w, "down_w": down_w}


EPS = 1e-06
LIMIT = 7.0
ALPHA = 1.702

def rms_scale(rows, gain):
    mean_sq = lax.optimization_barrier(jnp.mean(rows * rows, axis=-1, keepdims=True))
    return rows * lax.rsqrt(mean_sq + EPS) * gain

def slot_tables(routes, weights, expert_ids, capacity):
    blocks, seqs, top = routes.shape
    flat = routes.reshape(blocks, seqs * top)
    order = jnp.arange(seqs * top, dtype=jnp.int32)
    same = (flat[:, None, :] == flat[:, :, None]) & (order[None, None, :] < order[None, :, None])
    rank = lax.optimization_barrier(jnp.sum(same.astype(jnp.int32), axis=2))
    match = flat[:, :, None] == expert_ids[None, None, :]
    hit = rank[:, :, None] == jnp.arange(capacity, dtype=jnp.int32)[None, None, :]
    table = (match[:, :, :, None] & hit[:, :, None, :]).astype(jnp.float32)
    table = table.reshape(blocks, seqs, top, expert_ids.shape[0], capacity)
    dispatch = lax.optimization_barrier(jnp.sum(table, axis=2))
    combine = lax.optimization_barrier(jnp.sum(table * weights[:, :, :, None, None], axis=2))
    return (dispatch, combine)

def reference(tokens, lengths, cache_keys, cache_values, attn_gain, q_first_w, q_second_w, k_first_w, k_second_w, value_w, mix_lambda, head_gain, out_w, ffn_gain, routes, route_logits, gate_w, up_w, down_w):
    wide = tokens.astype(jnp.float32)
    normed = rms_scale(wide, attn_gain).astype(jnp.bfloat16)
    seqs = tokens.shape[0]
    half = HEAD_DIM // 2
    scale = half ** (-0.5)

    def project(weight, size):
        return jnp.dot(normed, weight, preferred_element_type=jnp.float32).astype(jnp.bfloat16).reshape(seqs, HEADS, size)
    q_first = project(q_first_w, half)
    q_second = project(q_second_w, half)
    k_first = project(k_first_w, half)
    k_second = project(k_second_w, half)
    new_value = project(value_w, HEAD_DIM)
    valid = jnp.arange(CACHE, dtype=jnp.int32)[None, :] < lengths[:, None]
    outputs = []
    for head in range(HEADS):
        keys = cache_keys[:, :, head * HEAD_DIM:(head + 1) * HEAD_DIM].astype(jnp.float32)
        values = cache_values[:, :, head * HEAD_DIM:(head + 1) * HEAD_DIM].astype(jnp.float32)
        maps = []
        for query, own_key, start in ((q_first, k_first, 0), (q_second, k_second, half)):
            query_f = query[:, head].astype(jnp.float32)
            own_f = own_key[:, head].astype(jnp.float32)
            scores = jnp.einsum('sd,std->st', query_f, keys[:, :, start:start + half]) * scale
            own = lax.optimization_barrier(jnp.sum(query_f * own_f, axis=-1)) * scale
            scores = jnp.where(valid, scores, -jnp.inf)
            top = jnp.maximum(lax.optimization_barrier(jnp.max(scores, axis=-1)), own)
            raised = jnp.exp(scores - top[:, None])
            own_raised = jnp.exp(own - top)
            total = lax.optimization_barrier(jnp.sum(raised, axis=-1)) + own_raised
            maps.append((raised / total[:, None], own_raised / total))
        lam = mix_lambda[head]
        mixed_w = (maps[0][0] - lam * maps[1][0]).astype(jnp.bfloat16)
        own_w = (maps[0][1] - lam * maps[1][1]).astype(jnp.bfloat16)
        head_out = jnp.einsum('st,std->sd', mixed_w.astype(jnp.float32), values)
        head_out = head_out + own_w.astype(jnp.float32)[:, None] * new_value[:, head].astype(jnp.float32)
        outputs.append(rms_scale(head_out, head_gain).astype(jnp.bfloat16))
    attended = jnp.stack(outputs, axis=1).reshape(seqs, HEADS * HEAD_DIM)
    after = wide + jnp.dot(attended, out_w, preferred_element_type=jnp.float32)
    expert_in = rms_scale(after, ffn_gain).astype(jnp.bfloat16)
    weights = jax.nn.softmax(route_logits, axis=-1)
    dispatch, combine = slot_tables(routes.reshape(N_EP, SEQ_GRP, TOP), weights.reshape(N_EP, SEQ_GRP, TOP), jnp.arange(EXPERTS, dtype=jnp.int32), CAP)
    buffer = jnp.einsum('bsec,bsd->becd', dispatch, expert_in.reshape(N_EP, SEQ_GRP, D).astype(jnp.float32)).astype(jnp.bfloat16)
    stacked = jnp.transpose(buffer, (1, 0, 2, 3)).reshape(EXPERTS, N_EP * CAP, D)

    def one_expert(items):
        rows, w_gate, w_up, w_down = items
        gate = jnp.dot(rows, w_gate, preferred_element_type=jnp.float32)
        up = jnp.dot(rows, w_up, preferred_element_type=jnp.float32)
        bound_gate = jnp.minimum(gate, LIMIT)
        bound_up = jnp.clip(up, -LIMIT, LIMIT)
        hidden = ((bound_up + 1.0) * bound_gate * jax.nn.sigmoid(ALPHA * bound_gate)).astype(jnp.bfloat16)
        return jnp.dot(hidden, w_down, preferred_element_type=jnp.float32).astype(jnp.bfloat16)
    results = lax.map(one_expert, (stacked, gate_w, up_w, down_w)).reshape(EXPERTS, N_EP, CAP, D)
    moe = jnp.einsum('bsec,ebcd->bsd', combine, results.astype(jnp.float32), precision=lax.Precision.HIGHEST).reshape(seqs, D)
    return (after + moe).astype(jnp.bfloat16)
```

```python
import jax
import jax.numpy as jnp
from jax import lax
from jax.experimental import pallas as pl
from jax.experimental.pallas import tpu as pltpu
from jax.sharding import PartitionSpec as P

EPS = 1e-06
LIMIT = 7.0
ALPHA = 1.702
MESH = pl.DeviceIdType.MESH
F32 = jnp.float32
BF16 = jnp.bfloat16

SMALL = ("tokens", "lengths", "attn_gain", "mix_lambda", "head_gain", "ffn_gain", "routes", "route_logits")
PROJ = ("q_first_w", "q_second_w", "k_first_w", "k_second_w", "value_w")
LATE = ("out_w", "gate_w", "up_w", "down_w")
CHUNKS = 4


def dot(a, b):
    return jnp.dot(a, b, preferred_element_type=F32)


def dot_nt(a, b):
    return lax.dot_general(a, b, (((1,), (1,)), ((), ())), preferred_element_type=F32)


def dot_tn(a, b):
    return lax.dot_general(a, b, (((0,), (0,)), ((), ())), preferred_element_type=F32)


def iota(shape, dim):
    return lax.broadcasted_iota(jnp.int32, shape, dim)


def load_plan(hbm, vm, sems):
    plan = {}
    for name in SMALL + PROJ:
        plan[name] = pltpu.make_async_copy(hbm[name], vm[name], sems.at[len(plan)])
    rows = hbm["cache_keys"].shape[1] // CHUNKS
    seqs = hbm["cache_keys"].shape[0] // CHUNKS
    for i in range(CHUNKS):
        part = pl.ds(i * rows, rows)
        plan["keys", i] = pltpu.make_async_copy(
            hbm["cache_keys"].at[:, part, :], vm["cache_keys"].at[:, part, :], sems.at[len(plan)]
        )
    for i in range(CHUNKS):
        part = pl.ds(i * seqs, seqs)
        plan["values", i] = pltpu.make_async_copy(
            hbm["cache_values"].at[part], vm["cache_values"].at[part], sems.at[len(plan)]
        )
    for name in LATE:
        plan[name] = pltpu.make_async_copy(hbm[name], vm[name], sems.at[len(plan)])
    return plan


N_LOADS = len(SMALL + PROJ + LATE) + 2 * CHUNKS


def attend(plan, vm, qbd, scores, wt, len_row, part_ref):
    for name in ("tokens", "attn_gain", "lengths", "mix_lambda", "head_gain"):
        plan[name].wait()
    seqs, width = vm["tokens"].shape
    length, dim = vm["cache_keys"].shape[1:]
    half = dim // 2
    tok = vm["tokens"][...].astype(F32)
    mean_sq = jnp.mean(tok * tok, axis=1, keepdims=True)
    normed = (tok * lax.rsqrt(mean_sq + EPS) * vm["attn_gain"][...]).astype(BF16)
    len_row[...] = jnp.zeros_like(len_row)
    len_row[0:1, 0:seqs] = vm["lengths"][...]

    def project(name):
        plan[name].wait()
        return dot(normed, vm[name][...]).astype(BF16)

    pad = jnp.zeros((dim - seqs, half), BF16)
    row = iota((dim, half), 0)
    col = iota((dim, half), 1)
    upper = (row == col).astype(F32).astype(BF16)
    lower = (row == col + half).astype(F32).astype(BF16)

    def columns(first, second):
        return dot_nt(upper, jnp.concatenate([first, pad], axis=0)) + dot_nt(
            lower, jnp.concatenate([second, pad], axis=0)
        )

    q_t = columns(project("q_first_w"), project("q_second_w")) * (half ** (-0.5))
    d_row = iota((dim, dim), 0)
    d_col = iota((dim, dim), 1)
    q_a = jnp.where(d_row < half, q_t, 0.0)
    q_b = jnp.where(d_row < half, 0.0, q_t)
    for s in range(seqs):
        mine = d_col == s
        qbd[s * dim : (s + 1) * dim, 0:dim] = jnp.where(mine, q_a, 0.0).astype(BF16)
        qbd[s * dim : (s + 1) * dim, dim : 2 * dim] = jnp.where(mine, q_b, 0.0).astype(BF16)
    k_t = columns(project("k_first_w"), project("k_second_w"))
    own = jnp.concatenate(
        [jnp.sum(q_a * k_t, axis=0, keepdims=True), jnp.sum(q_b * k_t, axis=0, keepdims=True)], axis=1
    )
    new_value = project("value_w").astype(F32)
    len_one = len_row[0:1, :]
    lens = jnp.concatenate([len_one, len_one], axis=1)
    rows = length // CHUNKS
    top = own
    for i in range(CHUNKS):
        plan["keys", i].wait()
        keys = jnp.concatenate(
            [vm["cache_keys"][s, i * rows : (i + 1) * rows, :] for s in range(seqs)], axis=1
        )
        got = dot(keys, qbd[...])
        valid = iota((rows, 2 * dim), 0) + i * rows < lens
        got = jnp.where(valid, got, -jnp.inf)
        scores[i * rows : (i + 1) * rows, :] = got
        top = jnp.maximum(top, jnp.max(got, axis=0, keepdims=True))
    own_raised = jnp.exp(own - top)
    total = own_raised
    for i in range(CHUNKS):
        raised = jnp.exp(scores[i * rows : (i + 1) * rows, :] - top)
        scores[i * rows : (i + 1) * rows, :] = raised
        total = total + jnp.sum(raised, axis=0, keepdims=True)
    inverse = 1.0 / total
    first = inverse[:, 0:dim]
    second = inverse[:, dim : 2 * dim] * vm["mix_lambda"][...]
    for i in range(length // dim):
        block = scores[i * dim : (i + 1) * dim, :]
        mixed = block[:, 0:dim] * first - block[:, dim : 2 * dim] * second
        wt[:, i * dim : (i + 1) * dim] = mixed.T[0:seqs, :].astype(BF16)
    own_w = own_raised[:, 0:dim] * first - own_raised[:, dim : 2 * dim] * second
    own_col = jnp.broadcast_to(own_w, (dim, dim)).T[0:seqs, :].astype(BF16).astype(F32)
    group = 16
    place = iota((group, dim), 0)
    outs = [jnp.zeros((group, dim), F32) for _ in range(seqs // group)]
    per = seqs // CHUNKS
    for i in range(CHUNKS):
        plan["values", i].wait()
        for s in range(i * per, (i + 1) * per, 2):
            g = s // group
            both = jnp.concatenate([vm["cache_values"][s], vm["cache_values"][s + 1]], axis=1)
            got = dot(wt[g * group : (g + 1) * group, :], both)
            outs[g] = outs[g] + jnp.where(place == s % group, got[:, 0:dim], 0.0)
            outs[g] = outs[g] + jnp.where(place == s % group + 1, got[:, dim : 2 * dim], 0.0)
    head_out = jnp.concatenate(outs, axis=0) + own_col * new_value
    mean_sq = jnp.mean(head_out * head_out, axis=1, keepdims=True)
    attended = (head_out * lax.rsqrt(mean_sq + EPS) * vm["head_gain"][...]).astype(BF16)
    plan["out_w"].wait()
    blocks, _, cols = part_ref.shape
    for b in range(blocks):
        part_ref[b] = dot(attended, vm["out_w"][:, b * cols : (b + 1) * cols]).astype(BF16)


def remote(src, dst, send, recv, ep, tp):
    return pltpu.make_async_remote_copy(
        src_ref=src, dst_ref=dst, send_sem=send, recv_sem=recv, device_id=(ep, tp), device_id_type=MESH
    )


def exchange(sizes, plan, vm, bufs, sems, out_ref):
    n_ep, n_tp, owned = sizes
    n_y = n_tp // 2
    e, t = lax.axis_index("ep"), lax.axis_index("tp")
    y, c = t // 2, t % 2
    partner = t + 1 - 2 * c
    part, rs, x1, x2, p1, p2, a1, a2, h2, hid, ret, fin = (bufs[k] for k in BUFS)
    seqs, cols = part.shape[1:]
    hc = cols // 2
    slots = n_ep * 16
    sent = []

    def send(*args):
        copy = remote(*args)
        copy.start()
        sent.append(copy)

    def arrive(buf, sem):
        remote(buf, buf, sems["idle"].at[0], sem, e, partner).wait_recv()

    for k in range(1, n_tp):
        to = (t + k) % n_tp
        send(part.at[to], rs.at[t], sems["rs_s"].at[k], sems["rs_r"].at[t], e, to)
    for name in ("routes", "route_logits", "ffn_gain"):
        plan[name].wait()
    routes, logits = vm["routes"][...], vm["route_logits"][...]
    logits = jnp.exp(logits - jnp.max(logits, axis=1, keepdims=True))
    weights = logits / jnp.sum(logits, axis=1, keepdims=True)
    slot = iota((seqs, slots), 1)
    named = jnp.zeros((seqs, slots), F32)
    weight = jnp.zeros((seqs, slots), F32)
    for k in range(routes.shape[1]):
        hit = routes[:, k : k + 1] == slot // 4
        named = jnp.where(hit, 1.0, named)
        weight = jnp.where(hit, weights[:, k : k + 1], weight)
    before = (iota((seqs, seqs), 1) < iota((seqs, seqs), 0)).astype(F32).astype(BF16)
    rank = dot(before, named.astype(BF16))
    taken = (named > 0.5) & (rank == (slot % 4).astype(F32))
    dispatch = jnp.where(taken, 1.0, 0.0).astype(BF16)
    combine = jnp.where(taken, weight, 0.0)
    combine_hi = combine.astype(BF16)
    combine_lo = (combine - combine_hi.astype(F32)).astype(BF16)
    start = pl.multiple_of(t * cols, cols)
    kept = vm["tokens"][:, pl.ds(start, cols)].astype(F32) + part[t].astype(F32)
    gain = vm["ffn_gain"][:, pl.ds(start, cols)]
    for k in range(1, n_tp):
        frm = (t + k) % n_tp
        arrive(rs.at[frm], sems["rs_r"].at[frm])
        kept = kept + rs[frm].astype(F32)
    ready = (kept * gain).astype(BF16)

    h2[y] = ready[:, hc:]
    for k in range(1, n_y):
        to = (t + 2 * k) % n_tp
        send(h2.at[y], h2.at[y], sems["h2_s"].at[k], sems["h2_r"].at[y], e, to)
    a1[...] = dot_tn(dispatch, ready[:, :hc]).astype(BF16).reshape(a1.shape)
    for k in range(1, n_ep):
        to = (e + k) % n_ep
        send(a1.at[to], x1.at[y, e], sems["x1_s"].at[k], sems["x1_r"].at[e], to, t)
    x1[y, e] = a1[e]
    for k in range(1, n_y):
        frm = (y + k) % n_y
        arrive(h2.at[frm], sems["h2_r"].at[frm])
    second = jnp.concatenate([h2[i] for i in range(n_y)], axis=1)
    a2[...] = dot_tn(dispatch, second).astype(BF16).reshape(a2.shape)
    for k in range(1, n_ep):
        to = (e + k) % n_ep
        send(a2.at[to], x2.at[e], sems["x2_s"].at[k], sems["x2_r"].at[e], to, t)
    x2[e] = a2[e]
    send(a2.at[e], p2.at[e], sems["d2_s"].at[0], sems["d2_r"].at[e], e, partner)
    for k in range(1, n_ep):
        frm = (e + k) % n_ep
        arrive(x1.at[y, frm], sems["x1_r"].at[frm])
    for k in range(1, n_y):
        to = (t + 2 * k) % n_tp
        send(x1.at[y], x1.at[y], sems["y1_s"].at[k], sems["y1_r"].at[y], e, to)
    send(x1.at[y], p1.at[y], sems["d1_s"].at[0], sems["d1_r"].at[y], e, partner)
    for k in range(1, n_y):
        frm = (y + k) % n_y
        arrive(x1.at[frm], sems["y1_r"].at[frm])
        send(x1.at[frm], p1.at[frm], sems["d1_s"].at[k], sems["d1_r"].at[frm], e, partner)
    for k in range(1, n_ep):
        frm = (e + n_ep - k) % n_ep
        arrive(x2.at[frm], sems["x2_r"].at[frm])
        send(x2.at[frm], p2.at[frm], sems["d2_s"].at[k], sems["d2_r"].at[frm], e, partner)

    for name in ("gate_w", "up_w", "down_w"):
        plan[name].wait()
    expert = iota((slots, 2 * vm["gate_w"].shape[2]), 0) % 16 // 4
    squares = jnp.zeros((slots, hc), F32)
    both = jnp.zeros(expert.shape, F32)
    back = 1.0 / vm["ffn_gain"][...]
    bufs["back"][...] = back * back
    for one, two, core in ((x1, x2, c), (p1, p2, 1 - c)):
        if one is p1:
            for i in range(n_y):
                arrive(p1.at[i], sems["d1_r"].at[i])
            for i in range(n_ep):
                arrive(p2.at[i], sems["d2_r"].at[i])
        spread = two[...].reshape(slots, n_y * hc)
        tiles, begins = [], []
        for i in range(n_y):
            begin = pl.multiple_of((2 * i + core) * cols, cols)
            begins.append(begin)
            a = one[i].reshape(slots, hc)
            b = spread[:, i * hc : (i + 1) * hc]
            tiles += [a, b]
            back_sq = bufs["back"][:, pl.ds(begin, cols)]
            squares = squares + a.astype(F32) * a.astype(F32) * back_sq[:, :hc]
            squares = squares + b.astype(F32) * b.astype(F32) * back_sq[:, hc:]
        rows_in = jnp.concatenate(tiles, axis=1)
        for j in range(owned):
            gates = jnp.concatenate([vm["gate_w"][j, pl.ds(b, cols), :] for b in begins], axis=0)
            ups = jnp.concatenate([vm["up_w"][j, pl.ds(b, cols), :] for b in begins], axis=0)
            got = dot(rows_in, jnp.concatenate([gates, ups], axis=1))
            both = both + jnp.where(expert == j, got, 0.0)
    scale = lax.rsqrt(jnp.sum(squares, axis=1, keepdims=True) / (n_tp * cols) + EPS)
    both = both * scale
    ff = vm["gate_w"].shape[2]
    gate = jnp.minimum(both[:, :ff], LIMIT)
    up = jnp.clip(both[:, ff:], -LIMIT, LIMIT)
    hid[t] = ((up + 1.0) * gate / (1.0 + jnp.exp(-ALPHA * gate))).astype(BF16)

    for k in range(1, n_y):
        to = (t + 2 * k) % n_tp
        send(hid.at[t], hid.at[t], sems["hy_s"].at[k], sems["hy_r"].at[y], e, to)
    send(hid.at[t], hid.at[t], sems["hd_s"].at[0], sems["hd_r"].at[y], e, partner)
    for k in range(1, n_y):
        frm = (y + k) % n_y
        block = hid.at[2 * frm + c]
        arrive(block, sems["hy_r"].at[frm])
        send(block, block, sems["hd_s"].at[k], sems["hd_r"].at[frm], e, partner)
    for i in range(n_y):
        arrive(hid.at[2 * i + 1 - c], sems["hd_r"].at[i])
    hidden = jnp.concatenate([hid[i] for i in range(n_tp)], axis=1)
    expert = iota((slots, cols), 0) % 16 // 4
    result = jnp.zeros((slots, cols), F32)
    for j in range(owned):
        result = result + jnp.where(expert == j, dot(hidden, vm["down_w"][j]), 0.0)
    ret[...] = result.astype(BF16).reshape(ret.shape)

    for k in range(1, n_ep):
        to = (e + k) % n_ep
        send(ret.at[to], fin.at[e], sems["re_s"].at[k], sems["re_r"].at[e], to, t)
    fin[e] = ret[e]
    for k in range(1, n_ep):
        frm = (e + n_ep - k) % n_ep
        arrive(fin.at[frm], sems["re_r"].at[frm])
    back_rows = fin[...].reshape(slots, cols)
    moe = dot(combine_hi, back_rows) + dot(combine_lo, back_rows)
    out_ref[...] = kept + moe
    for copy in sent:
        copy.wait_send()


BUFS = ("part", "rs", "x1", "x2", "p1", "p2", "a1", "a2", "h2", "hid", "ret", "fin")


def buffers(n_ep, n_tp, seqs, cols, ff):
    n_y, hc, slots = n_tp // 2, cols // 2, n_ep * 16
    v = lambda *shape: pltpu.VMEM(shape, BF16)
    return {
        "part": v(n_tp, seqs, cols),
        "rs": v(n_tp, seqs, cols),
        "x1": v(n_y, n_ep, 16, hc),
        "x2": v(n_ep, 16, n_y * hc),
        "p1": v(n_y, n_ep, 16, hc),
        "p2": v(n_ep, 16, n_y * hc),
        "a1": v(n_ep, 16, hc),
        "a2": v(n_ep, 16, n_y * hc),
        "h2": v(n_y, seqs, hc),
        "hid": v(n_tp, slots, ff),
        "ret": v(n_ep, 16, cols),
        "fin": v(n_ep, 16, cols),
        "back": pltpu.VMEM((1, n_tp * cols), F32),
    }


def semaphores(n_ep, n_tp):
    n_y = n_tp // 2
    d = lambda n: pltpu.SemaphoreType.DMA((n,))
    return {
        "idle": d(1),
        "rs_s": d(n_tp), "rs_r": d(n_tp),
        "h2_s": d(n_y), "h2_r": d(n_y),
        "x1_s": d(n_ep), "x1_r": d(n_ep),
        "x2_s": d(n_ep), "x2_r": d(n_ep),
        "y1_s": d(n_y), "y1_r": d(n_y),
        "d1_s": d(n_y), "d1_r": d(n_y),
        "d2_s": d(n_ep), "d2_r": d(n_ep),
        "hy_s": d(n_y), "hy_r": d(n_y),
        "hd_s": d(n_y), "hd_r": d(n_y),
        "re_s": d(n_ep), "re_r": d(n_ep),
    }


NAMES = (
    "tokens", "lengths", "cache_keys", "cache_values", "attn_gain", "q_first_w", "q_second_w", "k_first_w",
    "k_second_w", "value_w", "mix_lambda", "head_gain", "out_w", "ffn_gain", "routes", "route_logits",
    "gate_w", "up_w", "down_w",
)


def kernel_of(sizes, with_exchange=True):
    n_ep, n_tp, _ = sizes

    def kernel(hbm, out_ref, vm, attn_bufs, bufs, sems, load_sems):
        plan = load_plan(hbm, vm, load_sems)
        for copy in plan.values():
            copy.start()
        if with_exchange:
            e, t = lax.axis_index("ep"), lax.axis_index("tp")
            barrier = pltpu.get_barrier_semaphore()
            for k in range(1, n_tp):
                pl.semaphore_signal(barrier, inc=1, device_id=(e, (t + k) % n_tp), device_id_type=MESH)
            for k in range(1, n_ep):
                pl.semaphore_signal(barrier, inc=1, device_id=((e + k) % n_ep, t), device_id_type=MESH)
        attend(plan, vm, *attn_bufs, bufs["part"])
        if with_exchange:
            pl.semaphore_wait(barrier, n_tp + n_ep - 2)
            exchange(sizes, plan, vm, bufs, sems, out_ref)
        else:
            for name in ("routes", "route_logits", "ffn_gain", "gate_w", "up_w", "down_w"):
                plan[name].wait()
            for b in range(n_tp):
                out_ref[b] = bufs["part"][b].astype(F32)

    return kernel


def run(n_ep, n_tp, args, with_exchange=True):
    hbm = dict(zip(NAMES, args, strict=True))
    for name in ("lengths", "attn_gain", "mix_lambda", "head_gain", "ffn_gain"):
        hbm[name] = hbm[name].reshape(1, -1)
    seqs, width = hbm["tokens"].shape
    length, dim = hbm["cache_keys"].shape[1:]
    owned, _, ff = hbm["gate_w"].shape
    cols = width // n_tp
    vm = {name: pltpu.VMEM(x.shape, x.dtype) for name, x in hbm.items()}
    attn_bufs = [
        pltpu.VMEM((seqs * dim, 2 * dim), BF16),
        pltpu.VMEM((length, 2 * dim), F32),
        pltpu.VMEM((seqs, length), BF16),
        pltpu.VMEM((8, dim), jnp.int32),
    ]
    out = (seqs, cols) if with_exchange else (n_tp, seqs, cols)
    params = {"collective_id": 0, "has_side_effects": True} if with_exchange else {}
    return pl.pallas_call(
        kernel_of((n_ep, n_tp, owned), with_exchange),
        out_shape=jax.ShapeDtypeStruct(out, F32),
        in_specs=[{name: pl.BlockSpec(memory_space=pl.ANY) for name in hbm}],
        out_specs=pl.BlockSpec(memory_space=pltpu.VMEM),
        scratch_shapes=[
            vm, attn_bufs, buffers(n_ep, n_tp, seqs, cols, ff), semaphores(n_ep, n_tp),
            pltpu.SemaphoreType.DMA((N_LOADS,)),
        ],
        compiler_params=pltpu.CompilerParams(vmem_limit_bytes=56 * 1024 * 1024, **params),
    )(hbm)


def solution(mesh):
    n_ep, n_tp = mesh.shape["ep"], mesh.shape["tp"]

    def per_device(*args):
        return run(n_ep, n_tp, args).astype(BF16)

    return jax.shard_map(
        per_device,
        mesh=mesh,
        in_specs=(
            P("ep", None),
            P("ep"),
            P("ep", None, "tp"),
            P("ep", None, "tp"),
            P(),
            P(None, "tp"),
            P(None, "tp"),
            P(None, "tp"),
            P(None, "tp"),
            P(None, "tp"),
            P("tp"),
            P(),
            P("tp", None),
            P(),
            P("ep", None),
            P("ep", None),
            P("ep", None, "tp"),
            P("ep", None, "tp"),
            P("ep", None, "tp"),
        ),
        out_specs=P("ep", "tp"),
        check_vma=False,
    )
```

```python
from typing import Any, NamedTuple

import jax
import jax.numpy as jnp
from jax import lax
from jax.experimental import pallas as pl
from jax.experimental.pallas import tpu as pltpu
from jax.sharding import PartitionSpec as P

EPS = 1e-06
LIMIT = 7.0
ALPHA = 1.702
MESH = pl.DeviceIdType.MESH
F32 = jnp.float32
BF16 = jnp.bfloat16
CHUNKS = 4
ROWS = 16
scope = jax.named_scope


class Args(NamedTuple):
    tokens: Any
    lengths: Any
    cache_keys: Any
    cache_values: Any
    attn_gain: Any
    q_first_w: Any
    q_second_w: Any
    k_first_w: Any
    k_second_w: Any
    value_w: Any
    mix_lambda: Any
    head_gain: Any
    out_w: Any
    ffn_gain: Any
    routes: Any
    route_logits: Any
    gate_w: Any
    up_w: Any
    down_w: Any


class Held(NamedTuple):
    tokens: Any
    lengths: Any
    cache_keys: Any
    cache_values: Any
    attn_gain: Any
    narrow_w: Any
    value_w: Any
    mix_lambda: Any
    head_gain: Any
    out_w: Any
    ffn_gain: Any
    routes: Any
    route_logits: Any
    gate_up_w: Any
    down_w: Any


class Loads(NamedTuple):
    tokens: Any
    attn_gain: Any
    narrow_w: Any
    lengths: Any
    mix_lambda: Any
    head_gain: Any
    value_w: Any
    ffn_gain: Any
    routes: Any
    route_logits: Any
    keys: Any
    values: Any
    out_w: Any
    gate_up_w: Any
    down_w: Any


class Work(NamedTuple):
    queries: Any
    scores: Any
    mixed: Any
    len_row: Any
    narrow: Any


class Bufs(NamedTuple):
    part: Any
    rs: Any
    x1: Any
    x2: Any
    p1: Any
    p2: Any
    a1: Any
    a2: Any
    h2: Any
    hid: Any
    ret: Any
    fin: Any


class Pair(NamedTuple):
    send: Any
    recv: Any


class Sems(NamedTuple):
    idle: Any
    rs: Pair
    h2: Pair
    x1: Pair
    x2: Pair
    y1: Pair
    d1: Pair
    d2: Pair
    hy: Pair
    hd: Pair
    re: Pair


def dot(a, b):
    return jnp.dot(a, b, preferred_element_type=F32)


def dot_nt(a, b):
    return lax.dot_general(a, b, (((1,), (1,)), ((), ())), preferred_element_type=F32)


def iota(shape, dim):
    return lax.broadcasted_iota(jnp.int32, shape, dim)


def plan_loads(hbm, vm, sems):
    count = iter(range(N_LOADS))

    def copy(src, dst):
        return (pltpu.make_async_copy(src, dst, sems.at[next(count)]),)

    half = hbm.q_first_w.shape[0]
    rows = hbm.cache_keys.shape[1] // CHUNKS
    seqs = hbm.cache_keys.shape[0] // CHUNKS
    ff = hbm.gate_w.shape[2]
    narrow = (hbm.q_first_w, hbm.q_second_w, hbm.k_first_w, hbm.k_second_w)
    spans = [pl.ds(i * rows, rows) for i in range(CHUNKS)]
    blocks = [pl.ds(i * seqs, seqs) for i in range(CHUNKS)]
    return Loads(
        tokens=copy(hbm.tokens, vm.tokens),
        attn_gain=copy(hbm.attn_gain, vm.attn_gain),
        narrow_w=sum((copy(w, vm.narrow_w.at[pl.ds(i * half, half)]) for i, w in enumerate(narrow)), ()),
        lengths=copy(hbm.lengths, vm.lengths),
        mix_lambda=copy(hbm.mix_lambda, vm.mix_lambda),
        head_gain=copy(hbm.head_gain, vm.head_gain),
        value_w=copy(hbm.value_w, vm.value_w),
        ffn_gain=copy(hbm.ffn_gain, vm.ffn_gain),
        routes=copy(hbm.routes, vm.routes),
        route_logits=copy(hbm.route_logits, vm.route_logits),
        keys=sum((copy(hbm.cache_keys.at[:, s, :], vm.cache_keys.at[:, s, :]) for s in spans), ()),
        values=sum((copy(hbm.cache_values.at[b], vm.cache_values.at[b]) for b in blocks), ()),
        out_w=copy(hbm.out_w, vm.out_w),
        gate_up_w=copy(hbm.gate_w, vm.gate_up_w.at[:, :, pl.ds(0, ff)])
        + copy(hbm.up_w, vm.gate_up_w.at[:, :, pl.ds(ff, ff)]),
        down_w=copy(hbm.down_w, vm.down_w),
    )


N_LOADS = 17 + 2 * CHUNKS


def wait(copies):
    for copy in copies:
        copy.wait()


def attend(loads, vm, work, part_ref):
    with scope("load"):
        wait(loads.tokens + loads.attn_gain + loads.narrow_w + loads.lengths + loads.mix_lambda)
        wait(loads.head_gain + loads.value_w)
    with scope("proj"):
        seqs, width = vm.tokens.shape
        length, dim = vm.cache_keys.shape[1:]
        half = dim // 2
        tok = vm.tokens[...].astype(F32)
        mean_sq = jnp.mean(tok * tok, axis=1, keepdims=True)
        normed = (tok * lax.rsqrt(mean_sq + EPS) * vm.attn_gain[...]).astype(BF16)
        work.len_row[...] = jnp.zeros_like(work.len_row)
        work.len_row[0:1, 0:seqs] = vm.lengths[...]
        work.narrow[...] = jnp.zeros_like(work.narrow)
        work.narrow[:, 0:seqs] = dot_nt(vm.narrow_w[...], normed).astype(BF16).astype(F32)
        q_t = work.narrow[0:dim, :] * (half ** (-0.5))
        k_t = work.narrow[dim : 2 * dim, :]
        new_value = dot(normed, vm.value_w[...]).astype(BF16).astype(F32)
        d_row = iota((dim, dim), 0)
        d_col = iota((dim, dim), 1)
        q_a = jnp.where(d_row < half, q_t, 0.0)
        q_b = jnp.where(d_row < half, 0.0, q_t)
        for s in range(seqs):
            mine = d_col == s
            work.queries[s * dim : (s + 1) * dim, 0:dim] = jnp.where(mine, q_a, 0.0).astype(BF16)
            work.queries[s * dim : (s + 1) * dim, dim : 2 * dim] = jnp.where(mine, q_b, 0.0).astype(BF16)
        own = jnp.concatenate(
            [jnp.sum(q_a * k_t, axis=0, keepdims=True), jnp.sum(q_b * k_t, axis=0, keepdims=True)], axis=1
        )
        len_one = work.len_row[0:1, :]
        lens = jnp.concatenate([len_one, len_one], axis=1)
    rows = length // CHUNKS
    top = own
    for i in range(CHUNKS):
        with scope("wk"):
            loads.keys[i].wait()
        with scope("qk"):
            keys = jnp.concatenate(
                [vm.cache_keys[s, i * rows : (i + 1) * rows, :] for s in range(seqs)], axis=1
            )
            got = dot(keys, work.queries[...])
            valid = iota((rows, 2 * dim), 0) + i * rows < lens
            got = jnp.where(valid, got, -jnp.inf)
            work.scores[i * rows : (i + 1) * rows, :] = got
            top = jnp.maximum(top, jnp.max(got, axis=0, keepdims=True))
    with scope("soft"):
        own_raised = jnp.exp(own - top)
        total = own_raised
        for i in range(CHUNKS):
            raised = jnp.exp(work.scores[i * rows : (i + 1) * rows, :] - top)
            work.scores[i * rows : (i + 1) * rows, :] = raised
            total = total + jnp.sum(raised, axis=0, keepdims=True)
        inverse = 1.0 / total
        first = inverse[:, 0:dim]
        second = inverse[:, dim : 2 * dim] * vm.mix_lambda[...]
        for i in range(length // dim):
            block = work.scores[i * dim : (i + 1) * dim, :]
            mixed = block[:, 0:dim] * first - block[:, dim : 2 * dim] * second
            work.mixed[:, i * dim : (i + 1) * dim] = mixed.T[0:seqs, :].astype(BF16)
        own_w = own_raised[:, 0:dim] * first - own_raised[:, dim : 2 * dim] * second
        own_col = jnp.broadcast_to(own_w, (dim, dim)).T[0:seqs, :].astype(BF16).astype(F32)
    group = 16
    place = iota((group, dim), 0)
    outs = [jnp.zeros((group, dim), F32) for _ in range(seqs // group)]
    per = seqs // CHUNKS
    for i in range(CHUNKS):
        with scope("wv"):
            loads.values[i].wait()
        with scope("pv"):
            for s in range(i * per, (i + 1) * per, 2):
                g = s // group
                both = jnp.concatenate([vm.cache_values[s], vm.cache_values[s + 1]], axis=1)
                got = dot(work.mixed[g * group : (g + 1) * group, :], both)
                outs[g] = outs[g] + jnp.where(place == s % group, got[:, 0:dim], 0.0)
                outs[g] = outs[g] + jnp.where(place == s % group + 1, got[:, dim : 2 * dim], 0.0)
    with scope("head"):
        head_out = jnp.concatenate(outs, axis=0) + own_col * new_value
        mean_sq = jnp.mean(head_out * head_out, axis=1, keepdims=True)
        attended = (head_out * lax.rsqrt(mean_sq + EPS) * vm.head_gain[...]).astype(BF16)
        wait(loads.out_w)
        blocks, _, cols = part_ref.shape
        for b in range(blocks):
            part_ref[b] = dot(attended, vm.out_w[:, b * cols : (b + 1) * cols]).astype(BF16)


def remote(src, dst, send, recv, ep, tp):
    return pltpu.make_async_remote_copy(
        src_ref=src, dst_ref=dst, send_sem=send, recv_sem=recv, device_id=(ep, tp), device_id_type=MESH
    )


def slot_tables(vm, slots):
    routes, logits = vm.routes[...], vm.route_logits[...]
    top, seqs = routes.shape
    logits = jnp.exp(logits - jnp.max(logits, axis=0, keepdims=True))
    weights = logits / jnp.sum(logits, axis=0, keepdims=True)
    slot = iota((slots, seqs), 0)
    named = jnp.zeros((slots, seqs), F32)
    weight = jnp.zeros((slots, seqs), F32)
    for k in range(top):
        hit = routes[k : k + 1, :] == slot // 4
        named = jnp.where(hit, 1.0, named)
        weight = jnp.where(hit, weights[k : k + 1, :], weight)
    before = (iota((seqs, seqs), 0) < iota((seqs, seqs), 1)).astype(F32).astype(BF16)
    rank = dot(named.astype(BF16), before)
    taken = (named > 0.5) & (rank == (slot % 4).astype(F32))
    return jnp.where(taken, 1.0, 0.0).astype(BF16), jnp.where(taken, weight, 0.0)


def exchange(sizes, loads, vm, bufs, wide, sems, out_ref):
    n_ep, n_tp, owned = sizes
    n_y = n_tp // 2
    e, t = lax.axis_index("ep"), lax.axis_index("tp")
    y, c = t // 2, t % 2
    partner = t + 1 - 2 * c
    part, rs, x1, x2, p1, p2, a1, a2, h2, hid, ret, fin = bufs
    seqs, cols = part.shape[1:]
    hc = cols // 2
    slots = n_ep * ROWS
    sent = []

    def send(src, dst, pair, k, place, ep, tp):
        copy = remote(src, dst, pair.send.at[k], pair.recv.at[place], ep, tp)
        copy.start()
        sent.append(copy)

    def arrive(buf, pair, place):
        remote(buf, buf, sems.idle.at[0], pair.recv.at[place], e, partner).wait_recv()

    with scope("rs"):
        for k in range(1, n_tp):
            to = (t + k) % n_tp
            send(part.at[to], rs.at[t], sems.rs, k, t, e, to)
        wait(loads.routes + loads.route_logits + loads.ffn_gain)
        dispatch, combine = slot_tables(vm, slots)
        wide[...] = jnp.zeros_like(wide)
        wide[:, 0:seqs] = combine
        combine = jnp.concatenate([wide[i : i + 128, :].T[0:seqs, :] for i in range(0, slots, 128)], axis=1)
        combine_hi = combine.astype(BF16)
        combine_lo = (combine - combine_hi.astype(F32)).astype(BF16)
        start = pl.multiple_of(t * cols, cols)
        kept = vm.tokens[:, pl.ds(start, cols)].astype(F32) + part[t].astype(F32)
        gain = vm.ffn_gain[:, pl.ds(start, cols)]
    with scope("rsw"):
        for k in range(1, n_tp):
            frm = (t + k) % n_tp
            arrive(rs.at[frm], sems.rs, frm)
            kept = kept + rs[frm].astype(F32)
        ready = (kept * gain).astype(BF16)

    with scope("d1"):
        h2[y] = ready[:, hc:]
        for k in range(1, n_y):
            to = (t + 2 * k) % n_tp
            send(h2.at[y], h2.at[y], sems.h2, k, y, e, to)
        a1[...] = dot(dispatch, ready[:, :hc]).astype(BF16).reshape(a1.shape)
        for k in range(1, n_ep):
            to = (e + k) % n_ep
            send(a1.at[to], x1.at[y, e], sems.x1, k, e, to, t)
        x1[y, e] = a1[e]
    with scope("h2w"):
        for k in range(1, n_y):
            frm = (y + k) % n_y
            arrive(h2.at[frm], sems.h2, frm)
    with scope("d2"):
        second = jnp.concatenate([h2[i] for i in range(n_y)], axis=1)
        a2[...] = dot(dispatch, second).astype(BF16).reshape(a2.shape)
        for k in range(1, n_ep):
            to = (e + k) % n_ep
            send(a2.at[to], x2.at[e], sems.x2, k, e, to, t)
        x2[e] = a2[e]
        send(a2.at[e], p2.at[e], sems.d2, 0, e, e, partner)
    with scope("x1w"):
        for k in range(1, n_ep):
            frm = (e + k) % n_ep
            arrive(x1.at[y, frm], sems.x1, frm)
        for k in range(1, n_y):
            to = (t + 2 * k) % n_tp
            send(x1.at[y], x1.at[y], sems.y1, k, y, e, to)
        send(x1.at[y], p1.at[y], sems.d1, 0, y, e, partner)
    with scope("y1w"):
        for k in range(1, n_y):
            frm = (y + k) % n_y
            arrive(x1.at[frm], sems.y1, frm)
            send(x1.at[frm], p1.at[frm], sems.d1, k, frm, e, partner)
    with scope("x2w"):
        for k in range(1, n_ep):
            frm = (e + n_ep - k) % n_ep
            arrive(x2.at[frm], sems.x2, frm)
            send(x2.at[frm], p2.at[frm], sems.d2, k, frm, e, partner)

    wait(loads.gate_up_w + loads.down_w)
    ff = vm.gate_up_w.shape[2] // 2
    expert = iota((slots, 2 * ff), 0) % 16 // 4
    squares = jnp.zeros((slots, hc), F32)
    both = jnp.zeros((slots, 2 * ff), F32)
    for one, two, core in ((x1, x2, c), (p1, p2, 1 - c)):
        if one is p1:
            with scope("dw"):
                for i in range(n_y):
                    arrive(p1.at[i], sems.d1, i)
                for i in range(n_ep):
                    arrive(p2.at[i], sems.d2, i)
        with scope("gu"):
            spread = two[...].reshape(slots, n_y * hc)
            tiles, begins = [], []
            for i in range(n_y):
                begin = pl.multiple_of((2 * i + core) * cols, cols)
                begins.append(begin)
                a = one[i].reshape(slots, hc)
                b = spread[:, i * hc : (i + 1) * hc]
                tiles += [a, b]
                back = 1.0 / vm.ffn_gain[:, pl.ds(begin, cols)]
                a, b = a.astype(F32) * back[:, :hc], b.astype(F32) * back[:, hc:]
                squares = squares + a * a + b * b
            rows_in = jnp.concatenate(tiles, axis=1)
            for j in range(owned):
                w = jnp.concatenate([vm.gate_up_w[j, pl.ds(b, cols), :] for b in begins], axis=0)
                both = both + jnp.where(expert == j, dot(rows_in, w), 0.0)
    with scope("act"):
        scale = lax.rsqrt(jnp.sum(squares, axis=1, keepdims=True) / (n_tp * cols) + EPS)
        both = both * scale
        gate = jnp.minimum(both[:, :ff], LIMIT)
        up = jnp.clip(both[:, ff:], -LIMIT, LIMIT)
        hid[t] = ((up + 1.0) * gate / (1.0 + jnp.exp(-ALPHA * gate))).astype(BF16)

        for k in range(1, n_y):
            to = (t + 2 * k) % n_tp
            send(hid.at[t], hid.at[t], sems.hy, k, y, e, to)
        send(hid.at[t], hid.at[t], sems.hd, 0, y, e, partner)
    with scope("hyw"):
        for k in range(1, n_y):
            frm = (y + k) % n_y
            block = hid.at[2 * frm + c]
            arrive(block, sems.hy, frm)
            send(block, block, sems.hd, k, frm, e, partner)
    with scope("hdw"):
        for i in range(n_y):
            arrive(hid.at[2 * i + 1 - c], sems.hd, i)
    with scope("down"):
        hidden = jnp.concatenate([hid[i] for i in range(n_tp)], axis=1)
        expert = iota((slots, cols), 0) % 16 // 4
        result = jnp.zeros((slots, cols), F32)
        for j in range(owned):
            result = result + jnp.where(expert == j, dot(hidden, vm.down_w[j]), 0.0)
        ret[...] = result.astype(BF16).reshape(ret.shape)

        for k in range(1, n_ep):
            to = (e + k) % n_ep
            send(ret.at[to], fin.at[e], sems.re, k, e, to, t)
        fin[e] = ret[e]
    with scope("rew"):
        for k in range(1, n_ep):
            frm = (e + n_ep - k) % n_ep
            arrive(fin.at[frm], sems.re, frm)
    with scope("fin"):
        back_rows = fin[...].reshape(slots, cols)
        moe = dot(combine_hi, back_rows) + dot(combine_lo, back_rows)
        out_ref[...] = (kept + moe).astype(out_ref.dtype)
        for copy in sent:
            copy.wait_send()


def buffers(n_ep, n_tp, seqs, cols, ff):
    n_y, hc = n_tp // 2, cols // 2

    def array(*shape):
        return pltpu.VMEM(shape, BF16)

    return Bufs(
        part=array(n_tp, seqs, cols),
        rs=array(n_tp, seqs, cols),
        x1=array(n_y, n_ep, ROWS, hc),
        x2=array(n_ep, ROWS, n_y * hc),
        p1=array(n_y, n_ep, ROWS, hc),
        p2=array(n_ep, ROWS, n_y * hc),
        a1=array(n_ep, ROWS, hc),
        a2=array(n_ep, ROWS, n_y * hc),
        h2=array(n_y, seqs, hc),
        hid=array(n_tp, n_ep * ROWS, ff),
        ret=array(n_ep, ROWS, cols),
        fin=array(n_ep, ROWS, cols),
    )


def semaphores(n_ep, n_tp):
    n_y = n_tp // 2

    def pair(n):
        return Pair(pltpu.SemaphoreType.DMA((n,)), pltpu.SemaphoreType.DMA((n,)))

    return Sems(
        idle=pltpu.SemaphoreType.DMA((1,)),
        rs=pair(n_tp),
        h2=pair(n_y),
        x1=pair(n_ep),
        x2=pair(n_ep),
        y1=pair(n_y),
        d1=pair(n_y),
        d2=pair(n_ep),
        hy=pair(n_y),
        hd=pair(n_y),
        re=pair(n_ep),
    )


def run(n_ep, n_tp, hbm):
    seqs, width = hbm.tokens.shape
    length, dim = hbm.cache_keys.shape[1:]
    owned, _, ff = hbm.gate_w.shape
    cols = width // n_tp
    hbm = hbm._replace(
        lengths=hbm.lengths.reshape(1, -1),
        attn_gain=hbm.attn_gain.reshape(1, -1),
        head_gain=hbm.head_gain.reshape(1, -1),
        ffn_gain=hbm.ffn_gain.reshape(1, -1),
        mix_lambda=hbm.mix_lambda.reshape(1, -1),
        q_first_w=hbm.q_first_w.T,
        q_second_w=hbm.q_second_w.T,
        k_first_w=hbm.k_first_w.T,
        k_second_w=hbm.k_second_w.T,
        routes=hbm.routes.T,
        route_logits=hbm.route_logits.T,
    )

    def like(x):
        return pltpu.VMEM(x.shape, x.dtype)

    vm = Held(
        tokens=like(hbm.tokens),
        lengths=like(hbm.lengths),
        cache_keys=like(hbm.cache_keys),
        cache_values=like(hbm.cache_values),
        attn_gain=like(hbm.attn_gain),
        narrow_w=pltpu.VMEM((2 * dim, width), BF16),
        value_w=like(hbm.value_w),
        mix_lambda=like(hbm.mix_lambda),
        head_gain=like(hbm.head_gain),
        out_w=like(hbm.out_w),
        ffn_gain=like(hbm.ffn_gain),
        routes=like(hbm.routes),
        route_logits=like(hbm.route_logits),
        gate_up_w=pltpu.VMEM((owned, width, 2 * ff), BF16),
        down_w=like(hbm.down_w),
    )
    work = Work(
        queries=pltpu.VMEM((seqs * dim, 2 * dim), BF16),
        scores=pltpu.VMEM((length, 2 * dim), F32),
        mixed=pltpu.VMEM((seqs, length), BF16),
        len_row=pltpu.VMEM((8, dim), jnp.int32),
        narrow=pltpu.VMEM((2 * dim, dim), F32),
    )

    def kernel(hbm, out_ref, vm, work, bufs, wide, sems, load_sems):
        loads = plan_loads(hbm, vm, load_sems)
        for group in loads:
            for copy in group:
                copy.start()
        e, t = lax.axis_index("ep"), lax.axis_index("tp")
        barrier = pltpu.get_barrier_semaphore()
        for k in range(1, n_tp):
            pl.semaphore_signal(barrier, inc=1, device_id=(e, (t + k) % n_tp), device_id_type=MESH)
        for k in range(1, n_ep):
            pl.semaphore_signal(barrier, inc=1, device_id=((e + k) % n_ep, t), device_id_type=MESH)
        attend(loads, vm, work, bufs.part)
        with scope("bar"):
            pl.semaphore_wait(barrier, n_tp + n_ep - 2)
        exchange((n_ep, n_tp, owned), loads, vm, bufs, wide, sems, out_ref)

    return pl.pallas_call(
        kernel,
        out_shape=jax.ShapeDtypeStruct((seqs, cols), OUT),
        in_specs=[Args(*[pl.BlockSpec(memory_space=pl.ANY)] * len(hbm))],
        out_specs=pl.BlockSpec(memory_space=pltpu.VMEM),
        scratch_shapes=[
            vm,
            work,
            buffers(n_ep, n_tp, seqs, cols, ff),
            pltpu.VMEM((n_ep * ROWS, 128), F32),
            semaphores(n_ep, n_tp),
            pltpu.SemaphoreType.DMA((N_LOADS,)),
        ],
        compiler_params=pltpu.CompilerParams(
            vmem_limit_bytes=56 * 1024 * 1024, collective_id=0, has_side_effects=True
        ),
    )(hbm)


OUT = F32


def solution(mesh):
    n_ep, n_tp = mesh.shape["ep"], mesh.shape["tp"]

    def per_device(*args):
        return run(n_ep, n_tp, Args(*args)).astype(BF16)

    rows, heads, both = P("ep", None), P(None, "tp"), P("ep", None, "tp")
    return jax.shard_map(
        per_device,
        mesh=mesh,
        in_specs=(
            rows, P("ep"), both, both, P(), heads, heads, heads, heads, heads,
            P("tp"), P(), P("tp", None), P(), rows, rows, both, both, both,
        ),
        out_specs=P("ep", "tp"),
        check_vma=False,
    )
```

```python
from typing import Any, NamedTuple

import jax
import jax.numpy as jnp
from jax import lax
from jax.experimental import pallas as pl
from jax.experimental.pallas import tpu as pltpu
from jax.sharding import PartitionSpec as P

EPS = 1e-06
LIMIT = 7.0
ALPHA = 1.702
MESH = pl.DeviceIdType.MESH
F32 = jnp.float32
BF16 = jnp.bfloat16
CHUNKS = 4
KEY_CHUNKS = 4
ROWS = 16
scope = jax.named_scope


class Args(NamedTuple):
    tokens: Any
    lengths: Any
    cache_keys: Any
    cache_values: Any
    attn_gain: Any
    q_first_w: Any
    q_second_w: Any
    k_first_w: Any
    k_second_w: Any
    value_w: Any
    mix_lambda: Any
    head_gain: Any
    out_w: Any
    ffn_gain: Any
    routes: Any
    route_logits: Any
    gate_w: Any
    up_w: Any
    down_w: Any


class Held(NamedTuple):
    tokens: Any
    lengths: Any
    cache_keys: Any
    cache_values: Any
    attn_gain: Any
    narrow_w: Any
    value_w: Any
    mix_lambda: Any
    head_gain: Any
    out_w: Any
    ffn_gain: Any
    routes: Any
    route_logits: Any
    gate_up_w: Any
    down_w: Any


class Loads(NamedTuple):
    tokens: Any
    attn_gain: Any
    narrow_w: Any
    lengths: Any
    mix_lambda: Any
    head_gain: Any
    value_w: Any
    ffn_gain: Any
    routes: Any
    route_logits: Any
    keys: Any
    values: Any
    out_w: Any
    gate_up_w: Any
    down_w: Any


class Work(NamedTuple):
    queries: Any
    scores: Any
    mixed: Any
    len_row: Any
    narrow: Any


class Bufs(NamedTuple):
    part: Any
    rs: Any
    a: Any
    x: Any
    p: Any
    hid: Any
    ret: Any
    fin: Any


class Pair(NamedTuple):
    send: Any
    recv: Any


class Sems(NamedTuple):
    idle: Any
    rs: Pair
    x: Pair
    p: Pair
    hy: Pair
    hd: Pair
    re: Pair


def dot(a, b):
    return jnp.dot(a, b, preferred_element_type=F32)


def dot_nt(a, b):
    return lax.dot_general(a, b, (((1,), (1,)), ((), ())), preferred_element_type=F32)


def iota(shape, dim):
    return lax.broadcasted_iota(jnp.int32, shape, dim)


def plan_loads(hbm, vm, sems):
    count = iter(range(N_LOADS))

    def copy(src, dst):
        return (pltpu.make_async_copy(src, dst, sems.at[next(count)]),)

    half = hbm.q_first_w.shape[0]
    rows = hbm.cache_keys.shape[1] // KEY_CHUNKS
    seqs = hbm.cache_keys.shape[0] // CHUNKS
    ff = hbm.gate_w.shape[2]
    narrow = (hbm.q_first_w, hbm.q_second_w, hbm.k_first_w, hbm.k_second_w)
    spans = [pl.ds(i * rows, rows) for i in range(KEY_CHUNKS)]
    blocks = [pl.ds(i * seqs, seqs) for i in range(CHUNKS)]
    return Loads(
        tokens=copy(hbm.tokens, vm.tokens),
        attn_gain=copy(hbm.attn_gain, vm.attn_gain),
        narrow_w=sum((copy(w, vm.narrow_w.at[pl.ds(i * half, half)]) for i, w in enumerate(narrow)), ()),
        lengths=copy(hbm.lengths, vm.lengths),
        mix_lambda=copy(hbm.mix_lambda, vm.mix_lambda),
        head_gain=copy(hbm.head_gain, vm.head_gain),
        value_w=copy(hbm.value_w, vm.value_w),
        ffn_gain=copy(hbm.ffn_gain, vm.ffn_gain),
        routes=copy(hbm.routes, vm.routes),
        route_logits=copy(hbm.route_logits, vm.route_logits),
        keys=sum((copy(hbm.cache_keys.at[:, s, :], vm.cache_keys.at[:, s, :]) for s in spans), ()),
        values=sum((copy(hbm.cache_values.at[b], vm.cache_values.at[b]) for b in blocks), ()),
        out_w=copy(hbm.out_w, vm.out_w),
        gate_up_w=copy(hbm.gate_w, vm.gate_up_w.at[:, :, pl.ds(0, ff)])
        + copy(hbm.up_w, vm.gate_up_w.at[:, :, pl.ds(ff, ff)]),
        down_w=copy(hbm.down_w, vm.down_w),
    )


N_LOADS = 17 + KEY_CHUNKS + CHUNKS


def wait(copies):
    for copy in copies:
        copy.wait()


def attend(loads, vm, work, part_ref):
    with scope("load"):
        wait(loads.tokens + loads.attn_gain)
    with scope("proj"):
        seqs, width = vm.tokens.shape
        length, dim = vm.cache_keys.shape[1:]
        half = dim // 2
        tok = vm.tokens[...].astype(F32)
        mean_sq = jnp.mean(tok * tok, axis=1, keepdims=True)
        normed = (tok * lax.rsqrt(mean_sq + EPS) * vm.attn_gain[...]).astype(BF16)
        wait(loads.narrow_w)
        wait(loads.lengths + loads.mix_lambda + loads.head_gain + loads.value_w)
        work.len_row[...] = jnp.zeros_like(work.len_row)
        work.narrow[...] = jnp.zeros_like(work.narrow)
        narrow = dot_nt(vm.narrow_w[...], normed).astype(BF16).astype(F32)
        for i in range(4):
            lane = i % 2 * half
            work.narrow[i * half : (i + 1) * half, lane : lane + seqs] = narrow[i * half : (i + 1) * half, :]
        for lane in (0, half):
            work.len_row[0:1, lane : lane + seqs] = vm.lengths[...]
        q_t = work.narrow[0:dim, :] * (half ** (-0.5))
        k_t = work.narrow[dim : 2 * dim, :]
        new_value = dot(normed, vm.value_w[...]).astype(BF16).astype(F32)
        owner = iota((dim, dim), 1) - jnp.where(iota((dim, dim), 0) < half, 0, half)
        for s in range(seqs):
            work.queries[s * dim : (s + 1) * dim, :] = jnp.where(owner == s, q_t, 0.0).astype(BF16)
        own = jnp.sum(q_t * k_t, axis=0, keepdims=True)
        lens = work.len_row[0:1, :]
    rows = length // KEY_CHUNKS
    top = own
    for i in range(KEY_CHUNKS):
        with scope("wk"):
            loads.keys[i].wait()
        with scope("qk"):
            got = 0.0
            for first in range(0, seqs, seqs // 1):
                mine = range(first, first + seqs // 1)
                keys = jnp.concatenate([vm.cache_keys[s, i * rows : (i + 1) * rows, :] for s in mine], axis=1)
                got = got + dot(keys, work.queries[first * dim : (first + seqs // 1) * dim, :])
            valid = iota((rows, dim), 0) + i * rows < lens
            got = jnp.where(valid, got, -jnp.inf)
            work.scores[i * rows : (i + 1) * rows, :] = got
            top = jnp.maximum(top, jnp.max(got, axis=0, keepdims=True))
    with scope("soft"):
        own_raised = jnp.exp(own - top)
        total = own_raised
        for i in range(KEY_CHUNKS):
            raised = jnp.exp(work.scores[i * rows : (i + 1) * rows, :] - top)
            work.scores[i * rows : (i + 1) * rows, :] = raised
            total = total + jnp.sum(raised, axis=0, keepdims=True)
        share = jnp.where(iota((1, dim), 1) < half, 1.0, -vm.mix_lambda[...]) / total
        for i in range(length // dim):
            block = (work.scores[i * dim : (i + 1) * dim, :] * share).T
            mixed = block[0:seqs, :] + block[half : half + seqs, :]
            work.mixed[:, i * dim : (i + 1) * dim] = mixed.astype(BF16)
        own_w = jnp.broadcast_to(own_raised * share, (dim, dim)).T
        own_col = (own_w[0:seqs, :] + own_w[half : half + seqs, :]).astype(BF16).astype(F32)
    group = 16
    place = iota((group, dim), 0)
    outs = [jnp.zeros((group, dim), F32) for _ in range(seqs // group)]
    per = seqs // CHUNKS
    for i in range(CHUNKS):
        with scope("wv"):
            loads.values[i].wait()
        with scope("pv"):
            for s in range(i * per, (i + 1) * per, 2):
                g = s // group
                both = jnp.concatenate([vm.cache_values[s], vm.cache_values[s + 1]], axis=1)
                got = dot(work.mixed[g * group : (g + 1) * group, :], both)
                outs[g] = outs[g] + jnp.where(place == s % group, got[:, 0:dim], 0.0)
                outs[g] = outs[g] + jnp.where(place == s % group + 1, got[:, dim : 2 * dim], 0.0)
    with scope("head"):
        head_out = jnp.concatenate(outs, axis=0) + own_col * new_value
        mean_sq = jnp.mean(head_out * head_out, axis=1, keepdims=True)
        attended = (head_out * lax.rsqrt(mean_sq + EPS) * vm.head_gain[...]).astype(BF16)
        wait(loads.out_w)
        blocks, _, cols = part_ref.shape
        for b in range(blocks):
            part_ref[b] = dot(attended, vm.out_w[:, b * cols : (b + 1) * cols]).astype(BF16)


def remote(src, dst, send, recv, ep, tp):
    return pltpu.make_async_remote_copy(
        src_ref=src, dst_ref=dst, send_sem=send, recv_sem=recv, device_id=(ep, tp), device_id_type=MESH
    )


def slot_tables(vm, slots):
    routes, logits = vm.routes[...], vm.route_logits[...]
    top, seqs = routes.shape
    logits = jnp.exp(logits - jnp.max(logits, axis=0, keepdims=True))
    weights = logits / jnp.sum(logits, axis=0, keepdims=True)
    slot = iota((slots, seqs), 0)
    half = slots // 2
    expert = slot % half // 8 * 4 + slot // half * 2 + slot % 8 // 4
    named = jnp.zeros((slots, seqs), F32)
    weight = jnp.zeros((slots, seqs), F32)
    for k in range(top):
        hit = routes[k : k + 1, :] == expert
        named = jnp.where(hit, 1.0, named)
        weight = jnp.where(hit, weights[k : k + 1, :], weight)
    before = (iota((seqs, seqs), 0) < iota((seqs, seqs), 1)).astype(F32).astype(BF16)
    rank = dot(named.astype(BF16), before)
    taken = (named > 0.5) & (rank == (slot % 4).astype(F32))
    return jnp.where(taken, 1.0, 0.0).astype(BF16), jnp.where(taken, weight, 0.0)


def far_first(sizes):
    every = [()]
    for n in sizes:
        every = [o + (d,) for o in every for d in range(n)]
    hops = lambda o: sum(min(d, n - d) for d, n in zip(o, sizes, strict=True))
    return sorted(every, key=hops, reverse=True)


def exchange(sizes, loads, vm, bufs, wide, sems, out_ref):
    n_ep, n_tp, owned = sizes
    n_y, n_x = n_tp // 2, 4
    n_z = n_ep // n_x
    e, t = lax.axis_index("ep"), lax.axis_index("tp")
    y, c = t // 2, t % 2
    z, x = e // n_x, e % n_x
    partner = t + 1 - 2 * c
    seqs, cols = bufs.part.shape[1:]
    slots = n_ep * ROWS
    half = slots // 2
    lanes = 128

    def ep_at(dz, dx):
        return (z + dz) % n_z * n_x + (x + dx) % n_x

    def tp_at(dy, dc):
        return (y + dy) % n_y * 2 + (c + dc) % 2

    def send(src, dst, sent, got, ep, tp):
        remote(src, dst, sent, got, ep, tp).start()

    def sent_all(buf, sem):
        remote(buf, buf, sem, sems.idle.at[0], e, partner).wait_send()

    def arrive(buf, sem):
        remote(buf, buf, sems.idle.at[0], sem, e, partner).wait_recv()

    with scope("rs"):
        for dy, dc in far_first((n_y, 2)):
            if dy or dc:
                to = tp_at(dy, dc)
                send(bufs.part.at[to], bufs.rs.at[t], sems.rs.send.at[0], sems.rs.recv.at[0], e, to)
        wait(loads.routes + loads.route_logits + loads.ffn_gain)
        dispatch, combine = slot_tables(vm, slots)
        wide[...] = jnp.zeros_like(wide)
        wide[:, 0:seqs] = combine
        combine = jnp.concatenate([wide[i : i + lanes, :].T[0:seqs, :] for i in range(0, slots, lanes)], axis=1)
        combine_hi = combine.astype(BF16)
        combine_lo = (combine - combine_hi.astype(F32)).astype(BF16)
        start = pl.multiple_of(t * cols, cols)
        kept = vm.tokens[:, pl.ds(start, cols)].astype(F32)
        gain = vm.ffn_gain[:, pl.ds(start, cols)]
        bufs.rs[t] = bufs.part[t]
    with scope("rsw"):
        arrive(bufs.rs.at[pl.ds(0, n_tp - 1)], sems.rs.recv.at[0])
        for i in range(n_tp):
            kept = kept + bufs.rs[i].astype(F32)

    with scope("d1"):
        rows = dot(dispatch, (kept * gain).astype(BF16)).astype(BF16)
        bufs.a[...] = rows.reshape(bufs.a.shape)
        for dz, dx, dy in far_first((n_z, n_x, n_y)):
            to = ep_at(dz, dx)
            if dz or dx or dy:
                which = 1 if dy else 0
                send(
                    bufs.a.at[:, to], bufs.x.at[:, y, e], sems.x.send.at[which], sems.x.recv.at[e], to, tp_at(dy, 0)
                )
        bufs.x[:, y, e] = bufs.a[:, e]
    with scope("xw"):
        for dz, dx in reversed(far_first((n_z, n_x))):
            frm = ep_at(dz, dx)
            arrive(bufs.x.at[:, pl.ds(0, n_y if dz or dx else n_y - 1), frm], sems.x.recv.at[frm])
            send(bufs.x.at[:, :, frm], bufs.p.at[:, :, frm], sems.p.send.at[0], sems.p.recv.at[0], e, partner)

    wait(loads.gate_up_w + loads.down_w)
    ff = vm.gate_up_w.shape[2] // 2
    odd = iota((half, 2 * ff), 0) % 8 // 4 == 1

    def gate_up(buf, core, h):
        squares = jnp.zeros((half, lanes), F32)
        tiles, begins = [], []
        for i in range(n_y):
            begin = pl.multiple_of((2 * i + core) * cols, cols)
            begins.append(begin)
            tile = buf[h, i].reshape(half, cols)
            tiles.append(tile)
            tile = tile.astype(F32) * (1.0 / vm.ffn_gain[:, pl.ds(begin, cols)])
            for j in range(0, cols, lanes):
                squares = squares + tile[:, j : j + lanes] * tile[:, j : j + lanes]
        tiles = jnp.concatenate(tiles, axis=1)
        got = [
            dot(tiles, jnp.concatenate([vm.gate_up_w[j, pl.ds(b, cols), :] for b in begins], axis=0))
            for j in (2 * h, 2 * h + 1)
        ]
        return jnp.where(odd, got[1], got[0]), squares

    with scope("gu"):
        firsts = [gate_up(bufs.x, c, h) for h in range(2)]
    with scope("pw"):
        arrive(bufs.p, sems.p.recv.at[0])
    for h in range(2):
        with scope("gv"):
            both, squares = gate_up(bufs.p, 1 - c, h)
            both, squares = both + firsts[h][0], squares + firsts[h][1]
            scale = lax.rsqrt(jnp.sum(squares, axis=1, keepdims=True) / (n_tp * cols) + EPS)
            both = both * scale
            gate = jnp.minimum(both[:, :ff], LIMIT)
            up = jnp.clip(both[:, ff:], -LIMIT, LIMIT)
            mine = bufs.hid.at[h, t]
            mine[...] = ((up + 1.0) * gate / (1.0 + jnp.exp(-ALPHA * gate))).astype(BF16)

            for (dy,) in far_first((n_y,)):
                if dy:
                    send(mine, mine, sems.hy.send.at[h], sems.hy.recv.at[h * n_y + y], e, tp_at(dy, 0))
            send(mine, mine, sems.hd.send.at[h], sems.hd.recv.at[h], e, partner)
    odd = iota((half, cols), 0) % 8 // 4 == 1
    with scope("hyw"):
        for h in range(2):
            for (dy,) in reversed(far_first((n_y,))):
                if dy:
                    frm = tp_at(dy, 0)
                    block = bufs.hid.at[h, frm]
                    arrive(block, sems.hy.recv.at[h * n_y + frm // 2])
                    send(block, block, sems.hd.send.at[h], sems.hd.recv.at[h], e, partner)
    for h in range(2):
        with scope("hdw"):
            arrive(bufs.hid.at[h, pl.ds(0, n_y)], sems.hd.recv.at[h])
        with scope("down"):
            hidden = jnp.concatenate([bufs.hid[h, i] for i in range(n_tp)], axis=1)
            result = jnp.where(odd, dot(hidden, vm.down_w[2 * h + 1]), dot(hidden, vm.down_w[2 * h]))
            bufs.ret[h] = result.astype(BF16).reshape(bufs.ret.shape[1:])

            for dz, dx in far_first((n_z, n_x)):
                if dz or dx:
                    to = ep_at(dz, dx)
                    send(bufs.ret.at[h, to], bufs.fin.at[h, e], sems.re.send.at[h], sems.re.recv.at[h], to, t)
            bufs.fin[h, e] = bufs.ret[h, e]
    with scope("rew"):
        for h in range(2):
            arrive(bufs.fin.at[h, pl.ds(0, n_ep - 1)], sems.re.recv.at[h])
    with scope("fin"):
        back = bufs.fin[...].reshape(slots, cols)
        out_ref[...] = (kept + dot(combine_hi, back) + dot(combine_lo, back)).astype(out_ref.dtype)
        sent_all(bufs.part.at[pl.ds(0, n_tp - 1)], sems.rs.send.at[0])
        sent_all(bufs.x.at[:, 0, pl.ds(0, n_ep - 1)], sems.x.send.at[0])
        sent_all(bufs.x.at[:, pl.ds(0, n_y - 1)], sems.x.send.at[1])
        sent_all(bufs.x, sems.p.send.at[0])
        for h in range(2):
            sent_all(bufs.hid.at[h, pl.ds(0, n_y - 1)], sems.hy.send.at[h])
            sent_all(bufs.hid.at[h, pl.ds(0, n_y)], sems.hd.send.at[h])
            sent_all(bufs.ret.at[h, pl.ds(0, n_ep - 1)], sems.re.send.at[h])


def buffers(n_ep, n_tp, seqs, cols, ff):
    n_y, rows = n_tp // 2, ROWS // 2

    def array(*shape):
        return pltpu.VMEM(shape, BF16)

    return Bufs(
        part=array(n_tp, seqs, cols),
        rs=array(n_tp, seqs, cols),
        a=array(2, n_ep, rows, cols),
        x=array(2, n_y, n_ep, rows, cols),
        p=array(2, n_y, n_ep, rows, cols),
        hid=array(2, n_tp, n_ep * rows, ff),
        ret=array(2, n_ep, rows, cols),
        fin=array(2, n_ep, rows, cols),
    )


def semaphores(n_ep, n_tp):
    def pair(sends, recvs):
        return Pair(pltpu.SemaphoreType.DMA((sends,)), pltpu.SemaphoreType.DMA((recvs,)))

    return Sems(
        idle=pltpu.SemaphoreType.DMA((1,)),
        rs=pair(1, 1),
        x=pair(2, n_ep),
        p=pair(1, 1),
        hy=pair(2, n_tp),
        hd=pair(2, 2),
        re=pair(2, 2),
    )


def run(n_ep, n_tp, hbm):
    seqs, width = hbm.tokens.shape
    length, dim = hbm.cache_keys.shape[1:]
    owned, _, ff = hbm.gate_w.shape
    cols = width // n_tp
    hbm = hbm._replace(
        lengths=hbm.lengths.reshape(1, -1),
        attn_gain=hbm.attn_gain.reshape(1, -1),
        head_gain=hbm.head_gain.reshape(1, -1),
        ffn_gain=hbm.ffn_gain.reshape(1, -1),
        mix_lambda=hbm.mix_lambda.reshape(1, -1),
        q_first_w=hbm.q_first_w.T,
        q_second_w=hbm.q_second_w.T,
        k_first_w=hbm.k_first_w.T,
        k_second_w=hbm.k_second_w.T,
        routes=hbm.routes.T,
        route_logits=hbm.route_logits.T,
    )

    def like(x):
        return pltpu.VMEM(x.shape, x.dtype)

    vm = Held(
        tokens=like(hbm.tokens),
        lengths=like(hbm.lengths),
        cache_keys=like(hbm.cache_keys),
        cache_values=like(hbm.cache_values),
        attn_gain=like(hbm.attn_gain),
        narrow_w=pltpu.VMEM((2 * dim, width), BF16),
        value_w=like(hbm.value_w),
        mix_lambda=like(hbm.mix_lambda),
        head_gain=like(hbm.head_gain),
        out_w=like(hbm.out_w),
        ffn_gain=like(hbm.ffn_gain),
        routes=like(hbm.routes),
        route_logits=like(hbm.route_logits),
        gate_up_w=pltpu.VMEM((owned, width, 2 * ff), BF16),
        down_w=like(hbm.down_w),
    )
    work = Work(
        queries=pltpu.VMEM((seqs * dim, dim), BF16),
        scores=pltpu.VMEM((length, dim), F32),
        mixed=pltpu.VMEM((seqs, length), BF16),
        len_row=pltpu.VMEM((8, dim), jnp.int32),
        narrow=pltpu.VMEM((2 * dim, dim), F32),
    )

    def kernel(hbm, out_ref, vm, work, bufs, wide, sems, load_sems):
        loads = plan_loads(hbm, vm, load_sems)
        for group in loads:
            for copy in group:
                copy.start()
        e, t = lax.axis_index("ep"), lax.axis_index("tp")
        barrier = pltpu.get_barrier_semaphore()
        for k in range(1, n_tp):
            pl.semaphore_signal(barrier, inc=1, device_id=(e, (t + k) % n_tp), device_id_type=MESH)
        for k in range(1, n_ep):
            pl.semaphore_signal(barrier, inc=1, device_id=((e + k) % n_ep, t), device_id_type=MESH)
        attend(loads, vm, work, bufs.part)
        with scope("bar"):
            pl.semaphore_wait(barrier, n_tp + n_ep - 2)
        exchange((n_ep, n_tp, owned), loads, vm, bufs, wide, sems, out_ref)

    return pl.pallas_call(
        kernel,
        out_shape=pltpu.VMEM((seqs, cols), OUT),
        in_specs=[Args(*[pl.BlockSpec(memory_space=pl.ANY)] * len(hbm))],
        out_specs=pl.BlockSpec(memory_space=pltpu.VMEM),
        scratch_shapes=[
            vm,
            work,
            buffers(n_ep, n_tp, seqs, cols, ff),
            pltpu.VMEM((n_ep * ROWS, 128), F32),
            semaphores(n_ep, n_tp),
            pltpu.SemaphoreType.DMA((N_LOADS,)),
        ],
        compiler_params=pltpu.CompilerParams(
            vmem_limit_bytes=56 * 1024 * 1024, collective_id=0, has_side_effects=True
        ),
    )(hbm)


OUT = F32


def solution(mesh):
    n_ep, n_tp = mesh.shape["ep"], mesh.shape["tp"]

    def per_device(*args):
        return run(n_ep, n_tp, Args(*args)).astype(BF16)

    rows, heads, both = P("ep", None), P(None, "tp"), P("ep", None, "tp")
    return jax.shard_map(
        per_device,
        mesh=mesh,
        in_specs=(
            rows, P("ep"), both, both, P(), heads, heads, heads, heads, heads,
            P("tp"), P(), P("tp", None), P(), rows, rows, both, both, both,
        ),
        out_specs=P("ep", "tp"),
        check_vma=False,
    )
```

```python
from typing import Any, NamedTuple

import jax
import jax.numpy as jnp
from jax import lax
from jax.experimental import pallas as pl
from jax.experimental.pallas import tpu as pltpu
from jax.sharding import PartitionSpec as P

EPS = 1e-06
LIMIT = 7.0
ALPHA = 1.702
MESH = pl.DeviceIdType.MESH
F32 = jnp.float32
BF16 = jnp.bfloat16
CHUNKS = 2
KEY_CHUNKS = 4
ROWS = 16
EARLY = (0, 1, 2, 3, 4, 8)
scope = jax.named_scope


class Args(NamedTuple):
    tokens: Any
    lengths: Any
    cache_keys: Any
    cache_values: Any
    attn_gain: Any
    q_first_w: Any
    q_second_w: Any
    k_first_w: Any
    k_second_w: Any
    value_w: Any
    mix_lambda: Any
    head_gain: Any
    out_w: Any
    ffn_gain: Any
    routes: Any
    route_logits: Any
    gate_w: Any
    up_w: Any
    down_w: Any


class Held(NamedTuple):
    tokens: Any
    lengths: Any
    cache_keys: Any
    cache_values: Any
    attn_gain: Any
    narrow_w: Any
    value_w: Any
    mix_lambda: Any
    head_gain: Any
    out_w: Any
    ffn_gain: Any
    routes: Any
    route_logits: Any
    gate_up_w: Any
    down_w: Any


class Loads(NamedTuple):
    tokens: Any
    attn_gain: Any
    narrow_w: Any
    lengths: Any
    mix_lambda: Any
    head_gain: Any
    value_w: Any
    ffn_gain: Any
    routes: Any
    route_logits: Any
    keys: Any
    values: Any
    out_w: Any
    gate_up_w: Any
    down_w: Any


class Work(NamedTuple):
    queries: Any
    scores: Any
    mixed: Any
    len_row: Any
    narrow: Any


class Bufs(NamedTuple):
    part: Any
    rs: Any
    a: Any
    x: Any
    p: Any
    hid_a: Any
    hid_b: Any
    ret: Any
    fin: Any


class Pair(NamedTuple):
    send: Any
    recv: Any


class Sems(NamedTuple):
    idle: Any
    rs: Pair
    x: Pair
    p: Pair
    hy: Pair
    hd: Pair
    re: Pair


def dot(a, b):
    return jnp.dot(a, b, preferred_element_type=F32)


def dot_nt(a, b):
    return lax.dot_general(a, b, (((1,), (1,)), ((), ())), preferred_element_type=F32)


def iota(shape, dim):
    return lax.broadcasted_iota(jnp.int32, shape, dim)


class Pieces(NamedTuple):
    copies: Any
    whole: Any

    def start(self):
        for copy in self.copies:
            copy.start()

    def wait(self):
        self.whole.wait()


def plan_loads(hbm, vm, sems):
    count = iter(range(N_LOADS))

    def copy(src, dst):
        return (pltpu.make_async_copy(src, dst, sems.at[next(count)]),)

    def pieces(whole, parts):
        sem = sems.at[next(count)]
        return Pieces([pltpu.make_async_copy(s, d, sem) for s, d in parts], pltpu.make_async_copy(whole, whole, sem))

    half = hbm.q_first_w.shape[0]
    rows = hbm.cache_keys.shape[1] // KEY_CHUNKS
    seqs = hbm.cache_keys.shape[0] // CHUNKS
    ff = hbm.gate_w.shape[2]
    narrow = (hbm.q_first_w, hbm.q_second_w, hbm.k_first_w, hbm.k_second_w)
    spans = [pl.ds(i * rows, rows) for i in range(KEY_CHUNKS)]
    blocks = [pl.ds(i * seqs, seqs) for i in range(CHUNKS)]
    return Loads(
        tokens=copy(hbm.tokens, vm.tokens),
        attn_gain=copy(hbm.attn_gain, vm.attn_gain),
        narrow_w=(
            pieces(vm.narrow_w, [(w, vm.narrow_w.at[pl.ds(i * half, half)]) for i, w in enumerate(narrow)]),
        ),
        lengths=copy(hbm.lengths, vm.lengths),
        mix_lambda=copy(hbm.mix_lambda, vm.mix_lambda),
        head_gain=copy(hbm.head_gain, vm.head_gain),
        value_w=copy(hbm.value_w, vm.value_w),
        ffn_gain=copy(hbm.ffn_gain, vm.ffn_gain),
        routes=copy(hbm.routes, vm.routes),
        route_logits=copy(hbm.route_logits, vm.route_logits),
        keys=sum((copy(hbm.cache_keys.at[:, s, :], vm.cache_keys.at[:, s, :]) for s in spans), ()),
        values=sum((copy(hbm.cache_values.at[b], vm.cache_values.at[b]) for b in blocks), ()),
        out_w=copy(hbm.out_w, vm.out_w),
        gate_up_w=(
            pieces(
                vm.gate_up_w,
                [(hbm.gate_w, vm.gate_up_w.at[:, :, pl.ds(0, ff)]), (hbm.up_w, vm.gate_up_w.at[:, :, pl.ds(ff, ff)])],
            ),
        ),
        down_w=copy(hbm.down_w, vm.down_w),
    )


N_LOADS = 13 + KEY_CHUNKS + CHUNKS


def wait(copies):
    for copy in copies:
        copy.wait()


def attend(loads, vm, work, part_ref):
    with scope("load"):
        wait(loads.tokens + loads.attn_gain)
    with scope("proj"):
        seqs, width = vm.tokens.shape
        length, dim = vm.cache_keys.shape[1:]
        half = dim // 2
        tok = vm.tokens[...].astype(F32)
        mean_sq = jnp.mean(tok * tok, axis=1, keepdims=True)
        normed = (tok * lax.rsqrt(mean_sq + EPS) * vm.attn_gain[...]).astype(BF16)
        wait(loads.narrow_w)
        wait(loads.lengths)
        work.len_row[...] = jnp.zeros_like(work.len_row)
        work.narrow[...] = jnp.zeros_like(work.narrow)
        narrow = dot_nt(vm.narrow_w[...], normed).astype(BF16).astype(F32)
        for i in range(4):
            lane = i % 2 * half
            work.narrow[i * half : (i + 1) * half, lane : lane + seqs] = narrow[i * half : (i + 1) * half, :]
        for lane in (0, half):
            work.len_row[0:1, lane : lane + seqs] = vm.lengths[...]
        q_t = work.narrow[0:dim, :] * (half ** (-0.5))
        k_t = work.narrow[dim : 2 * dim, :]
        owner = iota((dim, dim), 1) - jnp.where(iota((dim, dim), 0) < half, 0, half)
        for s in range(seqs):
            work.queries[s * dim : (s + 1) * dim, :] = jnp.where(owner == s, q_t, 0.0).astype(BF16)
        own = jnp.sum(q_t * k_t, axis=0, keepdims=True)
        lens = work.len_row[0:1, :]
    rows = length // KEY_CHUNKS
    top = own
    for i in range(KEY_CHUNKS):
        with scope("wk"):
            loads.keys[i].wait()
        with scope("qk"):
            got = 0.0
            for first in range(0, seqs, seqs // 1):
                mine = range(first, first + seqs // 1)
                keys = jnp.concatenate([vm.cache_keys[s, i * rows : (i + 1) * rows, :] for s in mine], axis=1)
                got = got + dot(keys, work.queries[first * dim : (first + seqs // 1) * dim, :])
            valid = iota((rows, dim), 0) + i * rows < lens
            got = jnp.where(valid, got, -jnp.inf)
            work.scores[i * rows : (i + 1) * rows, :] = got
            top = jnp.maximum(top, jnp.max(got, axis=0, keepdims=True))
    with scope("soft"):
        wait(loads.mix_lambda + loads.value_w)
        new_value = dot(normed, vm.value_w[...]).astype(BF16).astype(F32)
        own_raised = jnp.exp(own - top)
        total = own_raised
        for i in range(KEY_CHUNKS):
            raised = jnp.exp(work.scores[i * rows : (i + 1) * rows, :] - top)
            work.scores[i * rows : (i + 1) * rows, :] = raised
            total = total + jnp.sum(raised, axis=0, keepdims=True)
        share = jnp.where(iota((1, dim), 1) < half, 1.0, -vm.mix_lambda[...]) / total
        for i in range(length // dim):
            block = (work.scores[i * dim : (i + 1) * dim, :] * share).T
            mixed = block[0:seqs, :] + block[half : half + seqs, :]
            work.mixed[:, i * dim : (i + 1) * dim] = mixed.astype(BF16)
        own_w = jnp.broadcast_to(own_raised * share, (dim, dim)).T
        own_col = (own_w[0:seqs, :] + own_w[half : half + seqs, :]).astype(BF16).astype(F32)
    group = 16
    place = iota((group, dim), 0)
    outs = [jnp.zeros((group, dim), F32) for _ in range(seqs // group)]
    per = seqs // CHUNKS
    for i in range(CHUNKS):
        with scope("wv"):
            loads.values[i].wait()
        with scope("pv"):
            for s in range(i * per, (i + 1) * per, 2):
                g = s // group
                both = jnp.concatenate([vm.cache_values[s], vm.cache_values[s + 1]], axis=1)
                got = dot(work.mixed[g * group : (g + 1) * group, :], both)
                outs[g] = outs[g] + jnp.where(place == s % group, got[:, 0:dim], 0.0)
                outs[g] = outs[g] + jnp.where(place == s % group + 1, got[:, dim : 2 * dim], 0.0)
    with scope("head"):
        wait(loads.head_gain)
        head_out = jnp.concatenate(outs, axis=0) + own_col * new_value
        mean_sq = jnp.mean(head_out * head_out, axis=1, keepdims=True)
        attended = (head_out * lax.rsqrt(mean_sq + EPS) * vm.head_gain[...]).astype(BF16)
        wait(loads.out_w)
        blocks, _, cols = part_ref.shape
        for b in range(blocks):
            part_ref[b] = dot(attended, vm.out_w[:, b * cols : (b + 1) * cols]).astype(BF16)


def remote(src, dst, send, recv, ep, tp):
    return pltpu.make_async_remote_copy(
        src_ref=src, dst_ref=dst, send_sem=send, recv_sem=recv, device_id=(ep, tp), device_id_type=MESH
    )


def slot_tables(vm, slots):
    routes, logits = vm.routes[...], vm.route_logits[...]
    top, seqs = routes.shape
    logits = jnp.exp(logits - jnp.max(logits, axis=0, keepdims=True))
    weights = logits / jnp.sum(logits, axis=0, keepdims=True)
    slot = iota((slots, seqs), 0)
    named = jnp.zeros((slots, seqs), F32)
    weight = jnp.zeros((slots, seqs), F32)
    for k in range(top):
        hit = routes[k : k + 1, :] == slot // 4
        named = jnp.where(hit, 1.0, named)
        weight = jnp.where(hit, weights[k : k + 1, :], weight)
    before = (iota((seqs, seqs), 0) < iota((seqs, seqs), 1)).astype(F32).astype(BF16)
    rank = dot(named.astype(BF16), before)
    taken = (named > 0.5) & (rank == (slot % 4).astype(F32))
    return jnp.where(taken, 1.0, 0.0).astype(BF16), jnp.where(taken, weight, 0.0)


def far_first(sizes):
    every = [()]
    for n in sizes:
        every = [o + (d,) for o in every for d in range(n)]
    hops = lambda o: sum(min(d, n - d) for d, n in zip(o, sizes, strict=True))
    return sorted(every, key=hops, reverse=True)


def exchange(sizes, loads, vm, bufs, wide, sems, out_ref):
    n_ep, n_tp, owned = sizes
    n_y, n_x = n_tp // 2, 4
    n_z = n_ep // n_x
    e, t = lax.axis_index("ep"), lax.axis_index("tp")
    y, c = t // 2, t % 2
    z, x = e // n_x, e % n_x
    partner = t + 1 - 2 * c
    seqs, cols = bufs.part.shape[1:]
    slots = n_ep * ROWS
    lanes = 128

    def ep_at(dz, dx):
        return (z + dz) % n_z * n_x + (x + dx) % n_x

    def tp_at(dy, dc):
        return (y + dy) % n_y * 2 + (c + dc) % 2

    def send(src, dst, sent, got, ep, tp):
        remote(src, dst, sent, got, ep, tp).start()

    def sent_all(buf, sem):
        remote(buf, buf, sem, sems.idle.at[0], e, partner).wait_send()

    def arrive(buf, sem):
        remote(buf, buf, sems.idle.at[0], sem, e, partner).wait_recv()

    with scope("rs"):
        for dy, dc in far_first((n_y, 2)):
            if dy or dc:
                to = tp_at(dy, dc)
                send(bufs.part.at[to], bufs.rs.at[t], sems.rs.send.at[0], sems.rs.recv.at[0], e, to)
        wait(loads.routes + loads.route_logits + loads.ffn_gain)
        dispatch, combine = slot_tables(vm, slots)
        wide[...] = jnp.zeros_like(wide)
        wide[:, 0:seqs] = combine
        combine = jnp.concatenate([wide[i : i + lanes, :].T[0:seqs, :] for i in range(0, slots, lanes)], axis=1)
        combine_hi = combine.astype(BF16)
        combine_lo = (combine - combine_hi.astype(F32)).astype(BF16)
        start = pl.multiple_of(t * cols, cols)
        kept = vm.tokens[:, pl.ds(start, cols)].astype(F32)
        gain = vm.ffn_gain[:, pl.ds(start, cols)]
        bufs.rs[t] = bufs.part[t]
    with scope("rsw"):
        arrive(bufs.rs.at[pl.ds(0, n_tp - 1)], sems.rs.recv.at[0])
        for i in range(n_tp):
            kept = kept + bufs.rs[i].astype(F32)

    with scope("d1"):
        rows = dot(dispatch, (kept * gain).astype(BF16)).astype(BF16)
        bufs.a[...] = rows.reshape(bufs.a.shape)
        for dz, dx, dy in far_first((n_z, n_x, n_y)):
            to = ep_at(dz, dx)
            if dz or dx or dy:
                which = 1 if dy else 0
                send(bufs.a.at[to], bufs.x.at[y, e], sems.x.send.at[which], sems.x.recv.at[e], to, tp_at(dy, 0))
        bufs.x[y, e] = bufs.a[e]

    halves = (EARLY, [g for g in range(n_ep) if g not in EARLY])
    hids = (bufs.hid_a, bufs.hid_b)
    ff = vm.gate_up_w.shape[2] // 2

    def of_expert(results):
        expert = iota(results[0].shape, 0) % ROWS // 4
        total = results[0]
        for j in range(1, owned):
            total = jnp.where(expert == j, results[j], total)
        return total

    def gate_up(buf, core, groups):
        squares = jnp.zeros((len(groups) * ROWS, lanes), F32)
        tiles, begins = [], []
        for i in range(n_y):
            begin = pl.multiple_of((2 * i + core) * cols, cols)
            begins.append(begin)
            tile = jnp.concatenate([buf[i, g] for g in groups], axis=0)
            tiles.append(tile)
            tile = tile.astype(F32) * (1.0 / vm.ffn_gain[:, pl.ds(begin, cols)])
            for j in range(0, cols, lanes):
                squares = squares + tile[:, j : j + lanes] * tile[:, j : j + lanes]
        tiles = jnp.concatenate(tiles, axis=1)
        got = [
            dot(tiles, jnp.concatenate([vm.gate_up_w[j, pl.ds(b, cols), :] for b in begins], axis=0))
            for j in range(owned)
        ]
        return of_expert(got), squares

    for h, groups in enumerate(halves):
        with scope("xw"):
            for g in groups:

                @pl.when(e != g)
                def _():
                    arrive(bufs.x.at[pl.ds(0, n_y), g], sems.x.recv.at[g])

                @pl.when(e == g)
                def _():
                    arrive(bufs.x.at[pl.ds(0, n_y - 1), g], sems.x.recv.at[g])

                send(bufs.x.at[:, g], bufs.p.at[:, g], sems.p.send.at[0], sems.p.recv.at[h], e, partner)
        if h == 0:
            wait(loads.gate_up_w + loads.down_w)
        with scope("gu"):
            first, first_squares = gate_up(bufs.x, c, groups)
        with scope("pw"):
            arrive(bufs.p.at[:, pl.ds(0, len(groups))], sems.p.recv.at[h])
        with scope("gv"):
            both, squares = gate_up(bufs.p, 1 - c, groups)
            both, squares = both + first, squares + first_squares
            scale = lax.rsqrt(jnp.sum(squares, axis=1, keepdims=True) / (n_tp * cols) + EPS)
            both = both * scale
            gate = jnp.minimum(both[:, :ff], LIMIT)
            up = jnp.clip(both[:, ff:], -LIMIT, LIMIT)
            mine = hids[h].at[t]
            mine[...] = ((up + 1.0) * gate / (1.0 + jnp.exp(-ALPHA * gate))).astype(BF16)

            for (dy,) in far_first((n_y,)):
                if dy:
                    send(mine, mine, sems.hy.send.at[h], sems.hy.recv.at[h * (n_y - 1) + dy - 1], e, tp_at(dy, 0))
            send(mine, mine, sems.hd.send.at[h], sems.hd.recv.at[h], e, partner)
    for h, groups in enumerate(halves):
        with scope("hyw"):
            for (dy,) in reversed(far_first((n_y,))):
                if dy:
                    frm = tp_at(dy, 0)
                    block = hids[h].at[frm]
                    arrive(block, sems.hy.recv.at[h * (n_y - 1) + n_y - dy - 1])
                    send(block, block, sems.hd.send.at[h], sems.hd.recv.at[h], e, partner)
        with scope("hdw"):
            arrive(hids[h].at[pl.ds(0, n_y)], sems.hd.recv.at[h])
        with scope("down"):
            hidden = jnp.concatenate([hids[h][i] for i in range(n_tp)], axis=1)
            result = of_expert([dot(hidden, vm.down_w[j]) for j in range(owned)]).astype(BF16)

            for i, g in enumerate(groups):
                bufs.ret[g] = result[i * ROWS : (i + 1) * ROWS, :]
            for g in reversed(groups):

                @pl.when(e != g)
                def _():
                    send(bufs.ret.at[g], bufs.fin.at[e], sems.re.send.at[0], sems.re.recv.at[0], g, t)

                @pl.when(e == g)
                def _():
                    bufs.fin[g] = bufs.ret[g]

    with scope("rew"):
        arrive(bufs.fin.at[pl.ds(0, n_ep - 1)], sems.re.recv.at[0])
    with scope("fin"):
        back = bufs.fin[...].reshape(slots, cols)
        out_ref[...] = (kept + dot(combine_hi, back) + dot(combine_lo, back)).astype(out_ref.dtype)
        sent_all(bufs.part.at[pl.ds(0, n_tp - 1)], sems.rs.send.at[0])
        sent_all(bufs.x.at[0, pl.ds(0, n_ep - 1)], sems.x.send.at[0])
        sent_all(bufs.x.at[pl.ds(0, n_y - 1)], sems.x.send.at[1])
        sent_all(bufs.x, sems.p.send.at[0])
        for h in range(2):
            sent_all(hids[h].at[pl.ds(0, n_y - 1)], sems.hy.send.at[h])
            sent_all(hids[h].at[pl.ds(0, n_y)], sems.hd.send.at[h])
        sent_all(bufs.ret.at[pl.ds(0, n_ep - 1)], sems.re.send.at[0])


def buffers(n_ep, n_tp, seqs, cols, ff):
    n_y = n_tp // 2

    def array(*shape):
        return pltpu.VMEM(shape, BF16)

    return Bufs(
        part=array(n_tp, seqs, cols),
        rs=array(n_tp, seqs, cols),
        a=array(n_ep, ROWS, cols),
        x=array(n_y, n_ep, ROWS, cols),
        p=array(n_y, n_ep, ROWS, cols),
        hid_a=array(n_tp, len(EARLY) * ROWS, ff),
        hid_b=array(n_tp, (n_ep - len(EARLY)) * ROWS, ff),
        ret=array(n_ep, ROWS, cols),
        fin=array(n_ep, ROWS, cols),
    )


def semaphores(n_ep, n_tp):
    def pair(sends, recvs):
        return Pair(pltpu.SemaphoreType.DMA((sends,)), pltpu.SemaphoreType.DMA((recvs,)))

    return Sems(
        idle=pltpu.SemaphoreType.DMA((1,)),
        rs=pair(1, 1),
        x=pair(2, n_ep),
        p=pair(1, 2),
        hy=pair(2, n_tp - 2),
        hd=pair(2, 2),
        re=pair(1, 1),
    )


def run(n_ep, n_tp, hbm):
    seqs, width = hbm.tokens.shape
    length, dim = hbm.cache_keys.shape[1:]
    owned, _, ff = hbm.gate_w.shape
    cols = width // n_tp
    hbm = hbm._replace(
        lengths=hbm.lengths.reshape(1, -1),
        attn_gain=hbm.attn_gain.reshape(1, -1),
        head_gain=hbm.head_gain.reshape(1, -1),
        ffn_gain=hbm.ffn_gain.reshape(1, -1),
        mix_lambda=hbm.mix_lambda.reshape(1, -1),
        q_first_w=hbm.q_first_w.T,
        q_second_w=hbm.q_second_w.T,
        k_first_w=hbm.k_first_w.T,
        k_second_w=hbm.k_second_w.T,
        routes=hbm.routes.T,
        route_logits=hbm.route_logits.T,
    )

    def like(x):
        return pltpu.VMEM(x.shape, x.dtype)

    vm = Held(
        tokens=like(hbm.tokens),
        lengths=like(hbm.lengths),
        cache_keys=like(hbm.cache_keys),
        cache_values=like(hbm.cache_values),
        attn_gain=like(hbm.attn_gain),
        narrow_w=pltpu.VMEM((2 * dim, width), BF16),
        value_w=like(hbm.value_w),
        mix_lambda=like(hbm.mix_lambda),
        head_gain=like(hbm.head_gain),
        out_w=like(hbm.out_w),
        ffn_gain=like(hbm.ffn_gain),
        routes=like(hbm.routes),
        route_logits=like(hbm.route_logits),
        gate_up_w=pltpu.VMEM((owned, width, 2 * ff), BF16),
        down_w=like(hbm.down_w),
    )
    work = Work(
        queries=pltpu.VMEM((seqs * dim, dim), BF16),
        scores=pltpu.VMEM((length, dim), F32),
        mixed=pltpu.VMEM((seqs, length), BF16),
        len_row=pltpu.VMEM((8, dim), jnp.int32),
        narrow=pltpu.VMEM((2 * dim, dim), F32),
    )

    def kernel(hbm, out_ref, vm, work, bufs, wide, sems, load_sems):
        loads = plan_loads(hbm, vm, load_sems)
        for group in loads:
            for copy in group:
                copy.start()
        e, t = lax.axis_index("ep"), lax.axis_index("tp")
        barrier = pltpu.get_barrier_semaphore()
        for k in range(1, n_tp):
            pl.semaphore_signal(barrier, inc=1, device_id=(e, (t + k) % n_tp), device_id_type=MESH)
        for k in range(1, n_ep):
            pl.semaphore_signal(barrier, inc=1, device_id=((e + k) % n_ep, t), device_id_type=MESH)
        attend(loads, vm, work, bufs.part)
        with scope("bar"):
            pl.semaphore_wait(barrier, n_tp + n_ep - 2)
        exchange((n_ep, n_tp, owned), loads, vm, bufs, wide, sems, out_ref)

    return pl.pallas_call(
        kernel,
        out_shape=pltpu.VMEM((seqs, cols), OUT),
        in_specs=[Args(*[pl.BlockSpec(memory_space=pl.ANY)] * len(hbm))],
        out_specs=pl.BlockSpec(memory_space=pltpu.VMEM),
        scratch_shapes=[
            vm,
            work,
            buffers(n_ep, n_tp, seqs, cols, ff),
            pltpu.VMEM((n_ep * ROWS, 128), F32),
            semaphores(n_ep, n_tp),
            pltpu.SemaphoreType.DMA((N_LOADS,)),
        ],
        compiler_params=pltpu.CompilerParams(
            vmem_limit_bytes=56 * 1024 * 1024, collective_id=0, has_side_effects=True
        ),
    )(hbm)


OUT = F32


def solution(mesh):
    n_ep, n_tp = mesh.shape["ep"], mesh.shape["tp"]

    def per_device(*args):
        return run(n_ep, n_tp, Args(*args)).astype(BF16)

    rows, heads, both = P("ep", None), P(None, "tp"), P("ep", None, "tp")
    return jax.shard_map(
        per_device,
        mesh=mesh,
        in_specs=(
            rows, P("ep"), both, both, P(), heads, heads, heads, heads, heads,
            P("tp"), P(), P("tp", None), P(), rows, rows, both, both, both,
        ),
        out_specs=P("ep", "tp"),
        check_vma=False,
    )
```

```python
from typing import Any, NamedTuple

import jax
import jax.numpy as jnp
from jax import lax
from jax.experimental import pallas as pl
from jax.experimental.pallas import tpu as pltpu
from jax.sharding import PartitionSpec as P

EPS = 1e-06
LIMIT = 7.0
ALPHA = 1.702
MESH = pl.DeviceIdType.MESH
F32 = jnp.float32
BF16 = jnp.bfloat16
CHUNKS = 2
KEY_CHUNKS = 4
ROWS = 16
EARLY = (0, 1, 2, 3, 4, 8)
scope = jax.named_scope


class Args(NamedTuple):
    tokens: Any
    lengths: Any
    cache_keys: Any
    cache_values: Any
    attn_gain: Any
    q_first_w: Any
    q_second_w: Any
    k_first_w: Any
    k_second_w: Any
    value_w: Any
    mix_lambda: Any
    head_gain: Any
    out_w: Any
    ffn_gain: Any
    routes: Any
    route_logits: Any
    gate_w: Any
    up_w: Any
    down_w: Any


class Held(NamedTuple):
    tokens: Any
    lengths: Any
    cache_keys: Any
    cache_values: Any
    attn_gain: Any
    narrow_w: Any
    value_w: Any
    mix_lambda: Any
    head_gain: Any
    out_w: Any
    ffn_gain: Any
    routes: Any
    route_logits: Any
    gate_up_w: Any
    down_w: Any


class Loads(NamedTuple):
    tokens: Any
    attn_gain: Any
    narrow_w: Any
    lengths: Any
    mix_lambda: Any
    head_gain: Any
    value_w: Any
    ffn_gain: Any
    routes: Any
    route_logits: Any
    keys: Any
    values: Any
    out_w: Any
    gate_up_w: Any
    down_w: Any


class Work(NamedTuple):
    queries: Any
    scores: Any
    mixed: Any
    len_row: Any
    narrow: Any


class Bufs(NamedTuple):
    part: Any
    rs: Any
    a: Any
    x: Any
    p: Any
    hid_a: Any
    hid_b: Any
    ret: Any
    fin: Any


class Pair(NamedTuple):
    send: Any
    recv: Any


class Sems(NamedTuple):
    idle: Any
    rs: Pair
    x: Pair
    p: Pair
    hy: Pair
    hd: Pair
    re: Pair


def dot(a, b):
    return jnp.dot(a, b, preferred_element_type=F32)


def dot_nt(a, b):
    return lax.dot_general(a, b, (((1,), (1,)), ((), ())), preferred_element_type=F32)


def iota(shape, dim):
    return lax.broadcasted_iota(jnp.int32, shape, dim)


class Pieces(NamedTuple):
    copies: Any
    whole: Any

    def start(self):
        for copy in self.copies:
            copy.start()

    def wait(self):
        self.whole.wait()


def plan_loads(hbm, vm, sems):
    count = iter(range(N_LOADS))

    def copy(src, dst):
        return (pltpu.make_async_copy(src, dst, sems.at[next(count)]),)

    def pieces(whole, parts):
        sem = sems.at[next(count)]
        return Pieces([pltpu.make_async_copy(s, d, sem) for s, d in parts], pltpu.make_async_copy(whole, whole, sem))

    half = hbm.q_first_w.shape[0]
    rows = hbm.cache_keys.shape[1] // KEY_CHUNKS
    seqs = hbm.cache_keys.shape[0] // CHUNKS
    ff = hbm.gate_w.shape[2]
    narrow = (hbm.q_first_w, hbm.q_second_w, hbm.k_first_w, hbm.k_second_w)
    spans = [pl.ds(i * rows, rows) for i in range(KEY_CHUNKS)]
    blocks = [pl.ds(i * seqs, seqs) for i in range(CHUNKS)]
    return Loads(
        tokens=copy(hbm.tokens, vm.tokens),
        attn_gain=copy(hbm.attn_gain, vm.attn_gain),
        narrow_w=(
            pieces(vm.narrow_w, [(w, vm.narrow_w.at[pl.ds(i * half, half)]) for i, w in enumerate(narrow)]),
        ),
        lengths=copy(hbm.lengths, vm.lengths),
        mix_lambda=copy(hbm.mix_lambda, vm.mix_lambda),
        head_gain=copy(hbm.head_gain, vm.head_gain),
        value_w=copy(hbm.value_w, vm.value_w),
        ffn_gain=copy(hbm.ffn_gain, vm.ffn_gain),
        routes=copy(hbm.routes, vm.routes),
        route_logits=copy(hbm.route_logits, vm.route_logits),
        keys=sum((copy(hbm.cache_keys.at[:, s, :], vm.cache_keys.at[:, s, :]) for s in spans), ()),
        values=sum((copy(hbm.cache_values.at[b], vm.cache_values.at[b]) for b in blocks), ()),
        out_w=copy(hbm.out_w, vm.out_w),
        gate_up_w=(
            pieces(
                vm.gate_up_w,
                [(hbm.gate_w, vm.gate_up_w.at[:, :, pl.ds(0, ff)]), (hbm.up_w, vm.gate_up_w.at[:, :, pl.ds(ff, ff)])],
            ),
        ),
        down_w=copy(hbm.down_w, vm.down_w),
    )


N_LOADS = 13 + KEY_CHUNKS + CHUNKS


def wait(copies):
    for copy in copies:
        copy.wait()


def attend(loads, vm, work, part_ref):
    with scope("load"):
        wait(loads.tokens + loads.attn_gain)
    with scope("proj"):
        seqs, width = vm.tokens.shape
        length, dim = vm.cache_keys.shape[1:]
        half = dim // 2
        tok = vm.tokens[...].astype(F32)
        mean_sq = jnp.mean(tok * tok, axis=1, keepdims=True)
        normed = (tok * lax.rsqrt(mean_sq + EPS) * vm.attn_gain[...]).astype(BF16)
        wait(loads.narrow_w)
        wait(loads.lengths)
        work.len_row[...] = jnp.zeros_like(work.len_row)
        work.narrow[...] = jnp.zeros_like(work.narrow)
        narrow = dot_nt(vm.narrow_w[...], normed).astype(BF16).astype(F32)
        for i in range(4):
            lane = i % 2 * half
            work.narrow[i * half : (i + 1) * half, lane : lane + seqs] = narrow[i * half : (i + 1) * half, :]
        for lane in (0, half):
            work.len_row[0:1, lane : lane + seqs] = vm.lengths[...]
        q_t = work.narrow[0:dim, :] * (half ** (-0.5))
        k_t = work.narrow[dim : 2 * dim, :]
        owner = iota((dim, dim), 1) - jnp.where(iota((dim, dim), 0) < half, 0, half)
        for s in range(seqs):
            work.queries[s * dim : (s + 1) * dim, :] = jnp.where(owner == s, q_t, 0.0).astype(BF16)
        own = jnp.sum(q_t * k_t, axis=0, keepdims=True)
        lens = work.len_row[0:1, :]
    rows = length // KEY_CHUNKS
    top = own
    for i in range(KEY_CHUNKS):
        with scope("wk"):
            loads.keys[i].wait()
        with scope("qk"):
            got = 0.0
            for first in range(0, seqs, seqs // 1):
                mine = range(first, first + seqs // 1)
                keys = jnp.concatenate([vm.cache_keys[s, i * rows : (i + 1) * rows, :] for s in mine], axis=1)
                got = got + dot(keys, work.queries[first * dim : (first + seqs // 1) * dim, :])
            valid = iota((rows, dim), 0) + i * rows < lens
            got = jnp.where(valid, got, -jnp.inf)
            work.scores[i * rows : (i + 1) * rows, :] = got
            top = jnp.maximum(top, jnp.max(got, axis=0, keepdims=True))
    with scope("soft"):
        wait(loads.mix_lambda + loads.value_w)
        new_value = dot(normed, vm.value_w[...]).astype(BF16).astype(F32)
        own_raised = jnp.exp(own - top)
        total = own_raised
        for i in range(KEY_CHUNKS):
            raised = jnp.exp(work.scores[i * rows : (i + 1) * rows, :] - top)
            work.scores[i * rows : (i + 1) * rows, :] = raised
            total = total + jnp.sum(raised, axis=0, keepdims=True)
        share = jnp.where(iota((1, dim), 1) < half, 1.0, -vm.mix_lambda[...]) / total
        for i in range(length // dim):
            block = (work.scores[i * dim : (i + 1) * dim, :] * share).T
            mixed = block[0:seqs, :] + block[half : half + seqs, :]
            work.mixed[:, i * dim : (i + 1) * dim] = mixed.astype(BF16)
        own_w = jnp.broadcast_to(own_raised * share, (dim, dim)).T
        own_col = (own_w[0:seqs, :] + own_w[half : half + seqs, :]).astype(BF16).astype(F32)
    group = 16
    place = iota((group, dim), 0)
    outs = [jnp.zeros((group, dim), F32) for _ in range(seqs // group)]
    per = seqs // CHUNKS
    for i in range(CHUNKS):
        with scope("wv"):
            loads.values[i].wait()
        with scope("pv"):
            for s in range(i * per, (i + 1) * per, 2):
                g = s // group
                both = jnp.concatenate([vm.cache_values[s], vm.cache_values[s + 1]], axis=1)
                got = dot(work.mixed[g * group : (g + 1) * group, :], both)
                outs[g] = outs[g] + jnp.where(place == s % group, got[:, 0:dim], 0.0)
                outs[g] = outs[g] + jnp.where(place == s % group + 1, got[:, dim : 2 * dim], 0.0)
    with scope("head"):
        wait(loads.head_gain)
        head_out = jnp.concatenate(outs, axis=0) + own_col * new_value
        mean_sq = jnp.mean(head_out * head_out, axis=1, keepdims=True)
        attended = (head_out * lax.rsqrt(mean_sq + EPS) * vm.head_gain[...]).astype(BF16)
        wait(loads.out_w)
        blocks, _, cols = part_ref.shape
        for b in range(blocks):
            part_ref[b] = dot(attended, vm.out_w[:, b * cols : (b + 1) * cols]).astype(BF16)


def remote(src, dst, send, recv, ep, tp):
    return pltpu.make_async_remote_copy(
        src_ref=src, dst_ref=dst, send_sem=send, recv_sem=recv, device_id=(ep, tp), device_id_type=MESH
    )


def slot_tables(vm, slots):
    routes, logits = vm.routes[...], vm.route_logits[...]
    top, seqs = routes.shape
    logits = jnp.exp(logits - jnp.max(logits, axis=0, keepdims=True))
    weights = logits / jnp.sum(logits, axis=0, keepdims=True)
    slot = iota((slots, seqs), 0)
    named = jnp.zeros((slots, seqs), F32)
    weight = jnp.zeros((slots, seqs), F32)
    for k in range(top):
        hit = routes[k : k + 1, :] == slot // 4
        named = jnp.where(hit, 1.0, named)
        weight = jnp.where(hit, weights[k : k + 1, :], weight)
    before = (iota((seqs, seqs), 0) < iota((seqs, seqs), 1)).astype(F32).astype(BF16)
    rank = dot(named.astype(BF16), before)
    taken = (named > 0.5) & (rank == (slot % 4).astype(F32))
    return jnp.where(taken, 1.0, 0.0).astype(BF16), jnp.where(taken, weight, 0.0)


def far_first(sizes):
    every = [()]
    for n in sizes:
        every = [o + (d,) for o in every for d in range(n)]
    hops = lambda o: sum(min(d, n - d) for d, n in zip(o, sizes, strict=True))
    return sorted(every, key=hops, reverse=True)


def exchange(sizes, loads, vm, bufs, wide, sems, out_ref):
    n_ep, n_tp, owned = sizes
    n_y, n_x = n_tp // 2, 4
    n_z = n_ep // n_x
    e, t = lax.axis_index("ep"), lax.axis_index("tp")
    y, c = t // 2, t % 2
    z, x = e // n_x, e % n_x
    partner = t + 1 - 2 * c
    seqs, cols = bufs.part.shape[1:]
    slots = n_ep * ROWS
    lanes = 128

    def ep_at(dz, dx):
        return (z + dz) % n_z * n_x + (x + dx) % n_x

    def tp_at(dy, dc):
        return (y + dy) % n_y * 2 + (c + dc + 2) % 2

    def send(src, dst, sent, got, ep, tp):
        remote(src, dst, sent, got, ep, tp).start()

    def sent_all(buf, sem):
        remote(buf, buf, sem, sems.idle.at[0], e, partner).wait_send()

    def arrive(buf, sem):
        remote(buf, buf, sems.idle.at[0], sem, e, partner).wait_recv()

    with scope("rs"):
        for dy, dc in far_first((n_y, 2)):
            if dy or dc:
                to = tp_at(dy, dc)
                send(bufs.part.at[to], bufs.rs.at[t], sems.rs.send.at[0], sems.rs.recv.at[0], e, to)
        wait(loads.routes + loads.route_logits + loads.ffn_gain)
        dispatch, combine = slot_tables(vm, slots)
        wide[...] = jnp.zeros_like(wide)
        wide[:, 0:seqs] = combine
        combine = jnp.concatenate([wide[i : i + lanes, :].T[0:seqs, :] for i in range(0, slots, lanes)], axis=1)
        combine_hi = combine.astype(BF16)
        combine_lo = (combine - combine_hi.astype(F32)).astype(BF16)
        start = pl.multiple_of(t * cols, cols)
        kept = vm.tokens[:, pl.ds(start, cols)].astype(F32)
        gain = vm.ffn_gain[:, pl.ds(start, cols)]
        bufs.rs[t] = bufs.part[t]
    with scope("rsw"):
        arrive(bufs.rs.at[pl.ds(0, n_tp - 1)], sems.rs.recv.at[0])
        for i in range(n_tp):
            kept = kept + bufs.rs[i].astype(F32)

    with scope("d1"):
        rows = dot(dispatch, (kept * gain).astype(BF16)).astype(BF16)
        bufs.a[...] = rows.reshape(bufs.a.shape)
        for dz, dx, dy in far_first((n_z, n_x, n_y)):
            to = ep_at(dz, dx)
            if dz or dx or dy:
                which = 1 if dy else 0
                send(bufs.a.at[to], bufs.x.at[y, e], sems.x.send.at[which], sems.x.recv.at[e], to, tp_at(dy, 0))
        bufs.x[y, e] = bufs.a[e]

    halves = (EARLY, [g for g in range(n_ep) if g not in EARLY])
    hids = (bufs.hid_a, bufs.hid_b)
    ff = vm.gate_up_w.shape[2] // 2

    def of_expert(results):
        expert = iota(results[0].shape, 0) % ROWS // 4
        total = results[0]
        for j in range(1, owned):
            total = jnp.where(expert == j, results[j], total)
        return total

    def gate_up(buf, core, groups):
        squares = jnp.zeros((len(groups) * ROWS, lanes), F32)
        tiles, begins = [], []
        for i in range(n_y):
            begin = pl.multiple_of((2 * i + core) * cols, cols)
            begins.append(begin)
            tile = jnp.concatenate([buf[i, g] for g in groups], axis=0)
            tiles.append(tile)
            tile = tile.astype(F32) * (1.0 / vm.ffn_gain[:, pl.ds(begin, cols)])
            for j in range(0, cols, lanes):
                squares = squares + tile[:, j : j + lanes] * tile[:, j : j + lanes]
        tiles = jnp.concatenate(tiles, axis=1)
        got = [
            dot(tiles, jnp.concatenate([vm.gate_up_w[j, pl.ds(b, cols), :] for b in begins], axis=0))
            for j in range(owned)
        ]
        return of_expert(got), squares

    for h, groups in enumerate(halves):
        with scope("xw"):
            for g in groups:

                @pl.when(e != g)
                def _():
                    arrive(bufs.x.at[pl.ds(0, n_y), g], sems.x.recv.at[g])

                @pl.when(e == g)
                def _():
                    arrive(bufs.x.at[pl.ds(0, n_y - 1), g], sems.x.recv.at[g])

                send(bufs.x.at[:, g], bufs.p.at[:, g], sems.p.send.at[0], sems.p.recv.at[h], e, partner)
        if h == 0:
            wait(loads.gate_up_w + loads.down_w)
        with scope("gu"):
            first, first_squares = gate_up(bufs.x, c, groups)
        with scope("pw"):
            arrive(bufs.p.at[:, pl.ds(0, len(groups))], sems.p.recv.at[h])
        with scope("gv"):
            both, squares = gate_up(bufs.p, 1 - c, groups)
            both, squares = both + first, squares + first_squares
            scale = lax.rsqrt(jnp.sum(squares, axis=1, keepdims=True) / (n_tp * cols) + EPS)
            both = both * scale
            gate = jnp.minimum(both[:, :ff], LIMIT)
            up = jnp.clip(both[:, ff:], -LIMIT, LIMIT)
            mine = hids[h].at[t]
            mine[...] = ((up + 1.0) * gate / (1.0 + jnp.exp(-ALPHA * gate))).astype(BF16)

            for (dy,) in far_first((n_y,)):
                if dy:
                    place = (h * (n_y - 1) + dy - 1) * 2 + c
                    send(mine, mine, sems.hy.send.at[h], sems.hy.recv.at[place], e, tp_at(dy, 1 - c))
            send(mine, mine, sems.hd.send.at[h], sems.hd.recv.at[h], e, partner)
    for h, groups in enumerate(halves):
        with scope("hyw"):

            @pl.when(c == 1)
            def _():
                for (dy,) in reversed(far_first((n_y,))):
                    for core in (1, 0) if dy else ():
                        block = hids[h].at[tp_at(dy, core - c)]
                        arrive(block, sems.hy.recv.at[(h * (n_y - 1) + n_y - dy - 1) * 2 + core])
                        send(block, block, sems.hd.send.at[h], sems.hd.recv.at[h], e, partner)
                arrive(hids[h].at[0], sems.hd.recv.at[h])

            @pl.when(c == 0)
            def _():
                arrive(hids[h].at[pl.ds(0, n_tp - 1)], sems.hd.recv.at[h])

        with scope("down"):
            hidden = jnp.concatenate([hids[h][i] for i in range(n_tp)], axis=1)
            result = of_expert([dot(hidden, vm.down_w[j]) for j in range(owned)]).astype(BF16)

            for i, g in enumerate(groups):
                bufs.ret[g] = result[i * ROWS : (i + 1) * ROWS, :]
            for g in reversed(groups):

                @pl.when(e != g)
                def _():
                    send(bufs.ret.at[g], bufs.fin.at[e], sems.re.send.at[0], sems.re.recv.at[0], g, t)

                @pl.when(e == g)
                def _():
                    bufs.fin[g] = bufs.ret[g]

    with scope("rew"):
        arrive(bufs.fin.at[pl.ds(0, n_ep - 1)], sems.re.recv.at[0])
    with scope("fin"):
        back = bufs.fin[...].reshape(slots, cols)
        out_ref[...] = (kept + dot(combine_hi, back) + dot(combine_lo, back)).astype(out_ref.dtype)
        sent_all(bufs.part.at[pl.ds(0, n_tp - 1)], sems.rs.send.at[0])
        sent_all(bufs.x.at[0, pl.ds(0, n_ep - 1)], sems.x.send.at[0])
        sent_all(bufs.x.at[pl.ds(0, n_y - 1)], sems.x.send.at[1])
        sent_all(bufs.x, sems.p.send.at[0])
        for h in range(2):
            sent_all(hids[h].at[pl.ds(0, n_y - 1)], sems.hy.send.at[h])

            @pl.when(c == 1)
            def _():
                sent_all(hids[h].at[pl.ds(0, n_tp - 1)], sems.hd.send.at[h])

            @pl.when(c == 0)
            def _():
                sent_all(hids[h].at[0], sems.hd.send.at[h])

        sent_all(bufs.ret.at[pl.ds(0, n_ep - 1)], sems.re.send.at[0])


def buffers(n_ep, n_tp, seqs, cols, ff):
    n_y = n_tp // 2

    def array(*shape):
        return pltpu.VMEM(shape, BF16)

    return Bufs(
        part=array(n_tp, seqs, cols),
        rs=array(n_tp, seqs, cols),
        a=array(n_ep, ROWS, cols),
        x=array(n_y, n_ep, ROWS, cols),
        p=array(n_y, n_ep, ROWS, cols),
        hid_a=array(n_tp, len(EARLY) * ROWS, ff),
        hid_b=array(n_tp, (n_ep - len(EARLY)) * ROWS, ff),
        ret=array(n_ep, ROWS, cols),
        fin=array(n_ep, ROWS, cols),
    )


def semaphores(n_ep, n_tp):
    def pair(sends, recvs):
        return Pair(pltpu.SemaphoreType.DMA((sends,)), pltpu.SemaphoreType.DMA((recvs,)))

    return Sems(
        idle=pltpu.SemaphoreType.DMA((1,)),
        rs=pair(1, 1),
        x=pair(2, n_ep),
        p=pair(1, 2),
        hy=pair(2, 2 * (n_tp - 2)),
        hd=pair(2, 2),
        re=pair(1, 1),
    )


def run(n_ep, n_tp, hbm):
    seqs, width = hbm.tokens.shape
    length, dim = hbm.cache_keys.shape[1:]
    owned, _, ff = hbm.gate_w.shape
    cols = width // n_tp
    hbm = hbm._replace(
        lengths=hbm.lengths.reshape(1, -1),
        attn_gain=hbm.attn_gain.reshape(1, -1),
        head_gain=hbm.head_gain.reshape(1, -1),
        ffn_gain=hbm.ffn_gain.reshape(1, -1),
        mix_lambda=hbm.mix_lambda.reshape(1, -1),
        q_first_w=hbm.q_first_w.T,
        q_second_w=hbm.q_second_w.T,
        k_first_w=hbm.k_first_w.T,
        k_second_w=hbm.k_second_w.T,
        routes=hbm.routes.T,
        route_logits=hbm.route_logits.T,
    )

    def like(x):
        return pltpu.VMEM(x.shape, x.dtype)

    vm = Held(
        tokens=like(hbm.tokens),
        lengths=like(hbm.lengths),
        cache_keys=like(hbm.cache_keys),
        cache_values=like(hbm.cache_values),
        attn_gain=like(hbm.attn_gain),
        narrow_w=pltpu.VMEM((2 * dim, width), BF16),
        value_w=like(hbm.value_w),
        mix_lambda=like(hbm.mix_lambda),
        head_gain=like(hbm.head_gain),
        out_w=like(hbm.out_w),
        ffn_gain=like(hbm.ffn_gain),
        routes=like(hbm.routes),
        route_logits=like(hbm.route_logits),
        gate_up_w=pltpu.VMEM((owned, width, 2 * ff), BF16),
        down_w=like(hbm.down_w),
    )
    work = Work(
        queries=pltpu.VMEM((seqs * dim, dim), BF16),
        scores=pltpu.VMEM((length, dim), F32),
        mixed=pltpu.VMEM((seqs, length), BF16),
        len_row=pltpu.VMEM((8, dim), jnp.int32),
        narrow=pltpu.VMEM((2 * dim, dim), F32),
    )

    def kernel(hbm, out_ref, vm, work, bufs, wide, sems, load_sems):
        loads = plan_loads(hbm, vm, load_sems)
        for group in loads:
            for copy in group:
                copy.start()
        e, t = lax.axis_index("ep"), lax.axis_index("tp")
        barrier = pltpu.get_barrier_semaphore()
        for k in range(1, n_tp):
            pl.semaphore_signal(barrier, inc=1, device_id=(e, (t + k) % n_tp), device_id_type=MESH)
        for k in range(1, n_ep):
            pl.semaphore_signal(barrier, inc=1, device_id=((e + k) % n_ep, t), device_id_type=MESH)
        attend(loads, vm, work, bufs.part)
        with scope("bar"):
            pl.semaphore_wait(barrier, n_tp + n_ep - 2)
        exchange((n_ep, n_tp, owned), loads, vm, bufs, wide, sems, out_ref)

    return pl.pallas_call(
        kernel,
        out_shape=pltpu.VMEM((seqs, cols), OUT),
        in_specs=[Args(*[pl.BlockSpec(memory_space=pl.ANY)] * len(hbm))],
        out_specs=pl.BlockSpec(memory_space=pltpu.VMEM),
        scratch_shapes=[
            vm,
            work,
            buffers(n_ep, n_tp, seqs, cols, ff),
            pltpu.VMEM((n_ep * ROWS, 128), F32),
            semaphores(n_ep, n_tp),
            pltpu.SemaphoreType.DMA((N_LOADS,)),
        ],
        compiler_params=pltpu.CompilerParams(
            vmem_limit_bytes=56 * 1024 * 1024, collective_id=0, has_side_effects=True
        ),
    )(hbm)


OUT = F32


def solution(mesh):
    n_ep, n_tp = mesh.shape["ep"], mesh.shape["tp"]

    def per_device(*args):
        return run(n_ep, n_tp, Args(*args)).astype(BF16)

    rows, heads, both = P("ep", None), P(None, "tp"), P("ep", None, "tp")
    return jax.shard_map(
        per_device,
        mesh=mesh,
        in_specs=(
            rows, P("ep"), both, both, P(), heads, heads, heads, heads, heads,
            P("tp"), P(), P("tp", None), P(), rows, rows, both, both, both,
        ),
        out_specs=P("ep", "tp"),
        check_vma=False,
    )
```

```python
import itertools
from typing import Any, NamedTuple

import jax
import jax.numpy as jnp
from jax import lax
from jax.experimental import pallas as pl
from jax.experimental.pallas import tpu as pltpu
from jax.sharding import PartitionSpec as P

EPS = 1e-06
LIMIT = 7.0
ALPHA = 1.702
MESH = pl.DeviceIdType.MESH
F32 = jnp.float32
BF16 = jnp.bfloat16
VALUE_CUTS = (0, 16, 28, 32)
KEY_CHUNKS = 4
ROWS = 16
SETS = ((0, 1, 2), (3, 4, 8)), ((5, 6, 7, 9), (10, 11, 12), (13, 14, 15))
EARLY = sum(SETS[0], ())
scope = jax.named_scope


class Args(NamedTuple):
    tokens: Any
    lengths: Any
    cache_keys: Any
    cache_values: Any
    attn_gain: Any
    q_first_w: Any
    q_second_w: Any
    k_first_w: Any
    k_second_w: Any
    value_w: Any
    mix_lambda: Any
    head_gain: Any
    out_w: Any
    ffn_gain: Any
    routes: Any
    route_logits: Any
    gate_w: Any
    up_w: Any
    down_w: Any


class Held(NamedTuple):
    tokens: Any
    lengths: Any
    cache_keys: Any
    cache_values: Any
    attn_gain: Any
    narrow_w: Any
    value_w: Any
    mix_lambda: Any
    head_gain: Any
    out_w: Any
    ffn_gain: Any
    routes: Any
    route_logits: Any
    gate_up_w: Any
    down_w: Any


class Loads(NamedTuple):
    tokens: Any
    attn_gain: Any
    narrow_w: Any
    lengths: Any
    mix_lambda: Any
    head_gain: Any
    value_w: Any
    ffn_gain: Any
    routes: Any
    route_logits: Any
    keys: Any
    values: Any
    out_w: Any
    gate_up_w: Any
    down_w: Any


class Work(NamedTuple):
    queries: Any
    scores: Any
    mixed: Any
    len_row: Any
    narrow: Any


class Bufs(NamedTuple):
    part: Any
    rs: Any
    a: Any
    x: Any
    p: Any
    hid_a: Any
    hid_b: Any
    ret: Any
    fin: Any


class Pair(NamedTuple):
    send: Any
    recv: Any


class Sems(NamedTuple):
    idle: Any
    rs: Pair
    x: Pair
    p: Pair
    hy: Pair
    hd: Pair
    re: Pair


def dot(a, b):
    return jnp.dot(a, b, preferred_element_type=F32)


def dot_nt(a, b):
    return lax.dot_general(a, b, (((1,), (1,)), ((), ())), preferred_element_type=F32)


def iota(shape, dim):
    return lax.broadcasted_iota(jnp.int32, shape, dim)


class Pieces(NamedTuple):
    copies: Any
    whole: Any

    def start(self):
        for copy in self.copies:
            copy.start()

    def wait(self):
        self.whole.wait()


def plan_loads(hbm, vm, sems):
    count = iter(range(N_LOADS))

    def copy(src, dst):
        return (pltpu.make_async_copy(src, dst, sems.at[next(count)]),)

    def pieces(whole, parts):
        sem = sems.at[next(count)]
        return Pieces([pltpu.make_async_copy(s, d, sem) for s, d in parts], pltpu.make_async_copy(whole, whole, sem))

    half = hbm.q_first_w.shape[0]
    rows = hbm.cache_keys.shape[1] // KEY_CHUNKS
    ff = hbm.gate_w.shape[2]
    narrow = (hbm.q_first_w, hbm.q_second_w, hbm.k_first_w, hbm.k_second_w)
    spans = [pl.ds(i * rows, rows) for i in range(KEY_CHUNKS)]
    blocks = [pl.ds(a, b - a) for a, b in itertools.pairwise(VALUE_CUTS)]
    return Loads(
        tokens=copy(hbm.tokens, vm.tokens),
        attn_gain=copy(hbm.attn_gain, vm.attn_gain),
        narrow_w=(
            pieces(vm.narrow_w, [(w, vm.narrow_w.at[pl.ds(i * half, half)]) for i, w in enumerate(narrow)]),
        ),
        lengths=copy(hbm.lengths, vm.lengths),
        mix_lambda=copy(hbm.mix_lambda, vm.mix_lambda),
        head_gain=copy(hbm.head_gain, vm.head_gain),
        value_w=copy(hbm.value_w, vm.value_w),
        ffn_gain=copy(hbm.ffn_gain, vm.ffn_gain),
        routes=copy(hbm.routes, vm.routes),
        route_logits=copy(hbm.route_logits, vm.route_logits),
        keys=sum((copy(hbm.cache_keys.at[:, s, :], vm.cache_keys.at[:, s, :]) for s in spans), ()),
        values=sum((copy(hbm.cache_values.at[b], vm.cache_values.at[b]) for b in blocks), ()),
        out_w=copy(hbm.out_w, vm.out_w),
        gate_up_w=(
            pieces(
                vm.gate_up_w,
                [(hbm.gate_w, vm.gate_up_w.at[:, :, pl.ds(0, ff)]), (hbm.up_w, vm.gate_up_w.at[:, :, pl.ds(ff, ff)])],
            ),
        ),
        down_w=copy(hbm.down_w, vm.down_w),
    )


N_LOADS = 12 + KEY_CHUNKS + len(VALUE_CUTS)


def wait(copies):
    for copy in copies:
        copy.wait()


def attend(loads, vm, work, part_ref):
    with scope("load"):
        wait(loads.tokens + loads.attn_gain)
    with scope("proj"):
        seqs, width = vm.tokens.shape
        length, dim = vm.cache_keys.shape[1:]
        half = dim // 2
        tok = vm.tokens[...].astype(F32)
        mean_sq = jnp.mean(tok * tok, axis=1, keepdims=True)
        normed = (tok * lax.rsqrt(mean_sq + EPS) * vm.attn_gain[...]).astype(BF16)
        wait(loads.narrow_w)
        wait(loads.lengths)
        work.len_row[...] = jnp.zeros_like(work.len_row)
        work.narrow[...] = jnp.zeros_like(work.narrow)
        narrow = dot_nt(vm.narrow_w[...], normed).astype(BF16).astype(F32)
        for i in range(4):
            lane = i % 2 * half
            work.narrow[i * half : (i + 1) * half, lane : lane + seqs] = narrow[i * half : (i + 1) * half, :]
        for lane in (0, half):
            work.len_row[0:1, lane : lane + seqs] = vm.lengths[...]
        q_t = work.narrow[0:dim, :] * (half ** (-0.5))
        k_t = work.narrow[dim : 2 * dim, :]
        owner = iota((dim, dim), 1) - jnp.where(iota((dim, dim), 0) < half, 0, half)
        for s in range(seqs):
            work.queries[s * dim : (s + 1) * dim, :] = jnp.where(owner == s, q_t, 0.0).astype(BF16)
        own = jnp.sum(q_t * k_t, axis=0, keepdims=True)
        lens = work.len_row[0:1, :]
    rows = length // KEY_CHUNKS
    top = own
    for i in range(KEY_CHUNKS):
        with scope("wk"):
            loads.keys[i].wait()
        with scope("qk"):
            got = 0.0
            for first in range(0, seqs, seqs // 1):
                mine = range(first, first + seqs // 1)
                keys = jnp.concatenate([vm.cache_keys[s, i * rows : (i + 1) * rows, :] for s in mine], axis=1)
                got = got + dot(keys, work.queries[first * dim : (first + seqs // 1) * dim, :])
            valid = iota((rows, dim), 0) + i * rows < lens
            got = jnp.where(valid, got, -jnp.inf)
            work.scores[i * rows : (i + 1) * rows, :] = got
            top = jnp.maximum(top, jnp.max(got, axis=0, keepdims=True))
    with scope("soft"):
        wait(loads.mix_lambda + loads.value_w)
        new_value = dot(normed, vm.value_w[...]).astype(BF16).astype(F32)
        own_raised = jnp.exp(own - top)
        total = own_raised
        for i in range(KEY_CHUNKS):
            raised = jnp.exp(work.scores[i * rows : (i + 1) * rows, :] - top)
            work.scores[i * rows : (i + 1) * rows, :] = raised
            total = total + jnp.sum(raised, axis=0, keepdims=True)
        share = jnp.where(iota((1, dim), 1) < half, 1.0, -vm.mix_lambda[...]) / total
        for i in range(length // dim):
            block = (work.scores[i * dim : (i + 1) * dim, :] * share).T
            mixed = block[0:seqs, :] + block[half : half + seqs, :]
            work.mixed[:, i * dim : (i + 1) * dim] = mixed.astype(BF16)
        own_w = jnp.broadcast_to(own_raised * share, (dim, dim)).T
        own_col = (own_w[0:seqs, :] + own_w[half : half + seqs, :]).astype(BF16).astype(F32)
    group = 16
    place = iota((group, dim), 0)
    outs = [jnp.zeros((group, dim), F32) for _ in range(seqs // group)]
    for i, (start, stop) in enumerate(itertools.pairwise(VALUE_CUTS)):
        with scope("wv"):
            loads.values[i].wait()
        with scope("pv"):
            for s in range(start, stop, 2):
                g = s // group
                both = jnp.concatenate([vm.cache_values[s], vm.cache_values[s + 1]], axis=1)
                got = dot(work.mixed[g * group : (g + 1) * group, :], both)
                outs[g] = outs[g] + jnp.where(place == s % group, got[:, 0:dim], 0.0)
                outs[g] = outs[g] + jnp.where(place == s % group + 1, got[:, dim : 2 * dim], 0.0)
    with scope("head"):
        wait(loads.head_gain)
        head_out = jnp.concatenate(outs, axis=0) + own_col * new_value
        mean_sq = jnp.mean(head_out * head_out, axis=1, keepdims=True)
        attended = (head_out * lax.rsqrt(mean_sq + EPS) * vm.head_gain[...]).astype(BF16)
        wait(loads.out_w)
        blocks, _, cols = part_ref.shape
        for b in range(blocks):
            part_ref[b] = dot(attended, vm.out_w[:, b * cols : (b + 1) * cols]).astype(BF16)


def remote(src, dst, send, recv, ep, tp):
    return pltpu.make_async_remote_copy(
        src_ref=src, dst_ref=dst, send_sem=send, recv_sem=recv, device_id=(ep, tp), device_id_type=MESH
    )


def slot_tables(vm, slots):
    routes, logits = vm.routes[...], vm.route_logits[...]
    top, seqs = routes.shape
    logits = jnp.exp(logits - jnp.max(logits, axis=0, keepdims=True))
    weights = logits / jnp.sum(logits, axis=0, keepdims=True)
    slot = iota((slots, seqs), 0)
    named = jnp.zeros((slots, seqs), F32)
    weight = jnp.zeros((slots, seqs), F32)
    for k in range(top):
        hit = routes[k : k + 1, :] == slot // 4
        named = jnp.where(hit, 1.0, named)
        weight = jnp.where(hit, weights[k : k + 1, :], weight)
    before = (iota((seqs, seqs), 0) < iota((seqs, seqs), 1)).astype(F32).astype(BF16)
    rank = dot(named.astype(BF16), before)
    taken = (named > 0.5) & (rank == (slot % 4).astype(F32))
    return jnp.where(taken, 1.0, 0.0).astype(BF16), jnp.where(taken, weight, 0.0)


def is_in(e, groups):
    return sum(1 // (1 + (e - g) * (e - g)) for g in groups)


def far_first(sizes):
    every = [()]
    for n in sizes:
        every = [o + (d,) for o in every for d in range(n)]
    hops = lambda o: sum(min(d, n - d) for d, n in zip(o, sizes, strict=True))
    return sorted(every, key=hops, reverse=True)


def exchange(sizes, loads, vm, bufs, wide, sems, out_ref):
    n_ep, n_tp, owned = sizes
    n_y, n_x = n_tp // 2, 4
    n_z = n_ep // n_x
    e, t = lax.axis_index("ep"), lax.axis_index("tp")
    y, c = t // 2, t % 2
    z, x = e // n_x, e % n_x
    partner = t + 1 - 2 * c
    seqs, cols = bufs.part.shape[1:]
    slots = n_ep * ROWS
    lanes = 128

    def ep_at(dz, dx):
        return (z + dz) % n_z * n_x + (x + dx) % n_x

    def tp_at(dy, dc):
        return (y + dy) % n_y * 2 + (c + dc + 2) % 2

    def send(src, dst, sent, got, ep, tp):
        remote(src, dst, sent, got, ep, tp).start()

    def sent_all(buf, sem):
        remote(buf, buf, sem, sems.idle.at[0], e, partner).wait_send()

    def arrive(buf, sem):
        remote(buf, buf, sems.idle.at[0], sem, e, partner).wait_recv()

    with scope("rs"):
        for dy, dc in far_first((n_y, 2)):
            if dy or dc:
                to = tp_at(dy, dc)
                send(bufs.part.at[to], bufs.rs.at[t], sems.rs.send.at[0], sems.rs.recv.at[0], e, to)
        wait(loads.routes + loads.route_logits + loads.ffn_gain)
        dispatch, combine = slot_tables(vm, slots)
        wide[...] = jnp.zeros_like(wide)
        wide[:, 0:seqs] = combine
        combine = jnp.concatenate([wide[i : i + lanes, :].T[0:seqs, :] for i in range(0, slots, lanes)], axis=1)
        combine_hi = combine.astype(BF16)
        combine_lo = (combine - combine_hi.astype(F32)).astype(BF16)
        start = pl.multiple_of(t * cols, cols)
        kept = vm.tokens[:, pl.ds(start, cols)].astype(F32)
        gain = vm.ffn_gain[:, pl.ds(start, cols)]
        bufs.rs[t] = bufs.part[t]
    with scope("rsw"):
        arrive(bufs.rs.at[pl.ds(0, n_tp - 1)], sems.rs.recv.at[0])
        for i in range(n_tp):
            kept = kept + bufs.rs[i].astype(F32)

    with scope("d1"):
        rows = dot(dispatch, (kept * gain).astype(BF16)).astype(BF16)
        bufs.a[...] = rows.reshape(bufs.a.shape)
        mine = sum(i * is_in(e, of) for i, of in enumerate(sum(SETS, ())))
        for dz, dx, dy in far_first((n_z, n_x, n_y)):
            to = ep_at(dz, dx)
            if dz or dx or dy:
                which = 1 if dy else 0
                send(bufs.a.at[to], bufs.x.at[y, e], sems.x.send.at[which], sems.x.recv.at[mine], to, tp_at(dy, 0))
        bufs.x[y, e] = bufs.a[e]

    halves = (EARLY, sum(SETS[1], ()))
    hids = (bufs.hid_a, bufs.hid_b)
    ff = vm.gate_up_w.shape[2] // 2

    def of_expert(results):
        expert = iota(results[0].shape, 0) % ROWS // 4
        total = results[0]
        for j in range(1, owned):
            total = jnp.where(expert == j, results[j], total)
        return total

    def gate_up(buf, core, groups):
        squares = jnp.zeros((len(groups) * ROWS, lanes), F32)
        tiles, begins = [], []
        for i in range(n_y):
            begin = pl.multiple_of((2 * i + core) * cols, cols)
            begins.append(begin)
            tile = jnp.concatenate([buf[i, g] for g in groups], axis=0)
            tiles.append(tile)
            tile = tile.astype(F32) * (1.0 / vm.ffn_gain[:, pl.ds(begin, cols)])
            for j in range(0, cols, lanes):
                squares = squares + tile[:, j : j + lanes] * tile[:, j : j + lanes]
        tiles = jnp.concatenate(tiles, axis=1)
        got = [
            dot(tiles, jnp.concatenate([vm.gate_up_w[j, pl.ds(b, cols), :] for b in begins], axis=0))
            for j in range(owned)
        ]
        return of_expert(got), squares

    def collect(h):
        for of in SETS[h]:
            place = sum(SETS, ()).index(of)
            copies = n_y * len(of)

            @pl.when(is_in(e, of) == 0)
            def _():
                arrive(bufs.x.at[0, pl.ds(0, copies)], sems.x.recv.at[place])

            @pl.when(is_in(e, of) == 1)
            def _():
                arrive(bufs.x.at[0, pl.ds(0, copies - 1)], sems.x.recv.at[place])

            for g in of:
                send(bufs.x.at[:, g], bufs.p.at[:, g], sems.p.send.at[0], sems.p.recv.at[h], e, partner)

    for h, groups in enumerate(halves):
        if h == 0:
            with scope("xw"):
                collect(0)
            wait(loads.gate_up_w + loads.down_w)
        else:
            with scope("xb"):
                pl.when(c == 0)(lambda: collect(1))
        with scope("gu"):
            first, first_squares = gate_up(bufs.x, c, groups)
        if h == 0:
            with scope("xc"):
                pl.when(c == 1)(lambda: collect(1))
        with scope("pw"):
            arrive(bufs.p.at[:, pl.ds(0, len(groups))], sems.p.recv.at[h])
        with scope("gv"):
            both, squares = gate_up(bufs.p, 1 - c, groups)
            both, squares = both + first, squares + first_squares
            scale = lax.rsqrt(jnp.sum(squares, axis=1, keepdims=True) / (n_tp * cols) + EPS)
            both = both * scale
            gate = jnp.minimum(both[:, :ff], LIMIT)
            up = jnp.clip(both[:, ff:], -LIMIT, LIMIT)
            mine = hids[h].at[t]
            mine[...] = ((up + 1.0) * gate / (1.0 + jnp.exp(-ALPHA * gate))).astype(BF16)

            for (dy,) in far_first((n_y,)):
                if dy:
                    place = h * (n_y - 1) + dy - 1
                    send(mine, mine, sems.hy.send.at[h], sems.hy.recv.at[place], e, tp_at(dy, 1 - c))
            send(mine, mine, sems.hd.send.at[h], sems.hd.recv.at[h], e, partner)
    for h, groups in enumerate(halves):
        with scope("hyw"):

            @pl.when(c == 1)
            def _():
                for (dy,) in reversed(far_first((n_y,))):
                    if dy:
                        block = hids[h].at[pl.ds((y + dy) % n_y * 2, 2)]
                        arrive(block, sems.hy.recv.at[h * (n_y - 1) + n_y - dy - 1])
                        send(block, block, sems.hd.send.at[h], sems.hd.recv.at[h], e, partner)
                arrive(hids[h].at[0], sems.hd.recv.at[h])

            @pl.when(c == 0)
            def _():
                arrive(hids[h].at[pl.ds(0, n_tp - 1)], sems.hd.recv.at[h])

        with scope("down"):
            hidden = jnp.concatenate([hids[h][i] for i in range(n_tp)], axis=1)
            result = of_expert([dot(hidden, vm.down_w[j]) for j in range(owned)]).astype(BF16)

            for i, g in enumerate(groups):
                bufs.ret[g] = result[i * ROWS : (i + 1) * ROWS, :]
            for g in reversed(groups):

                @pl.when(e != g)
                def _():
                    send(bufs.ret.at[g], bufs.fin.at[e], sems.re.send.at[0], sems.re.recv.at[0], g, t)

                @pl.when(e == g)
                def _():
                    bufs.fin[g] = bufs.ret[g]

    with scope("rew"):
        arrive(bufs.fin.at[pl.ds(0, n_ep - 1)], sems.re.recv.at[0])
    with scope("fin"):
        back = bufs.fin[...].reshape(slots, cols)
        out_ref[...] = (kept + dot(combine_hi, back) + dot(combine_lo, back)).astype(out_ref.dtype)
        sent_all(bufs.part.at[pl.ds(0, n_tp - 1)], sems.rs.send.at[0])
        sent_all(bufs.x.at[0, pl.ds(0, n_ep - 1)], sems.x.send.at[0])
        sent_all(bufs.x.at[pl.ds(0, n_y - 1)], sems.x.send.at[1])
        sent_all(bufs.x, sems.p.send.at[0])
        for h in range(2):
            sent_all(hids[h].at[pl.ds(0, n_y - 1)], sems.hy.send.at[h])

            @pl.when(c == 1)
            def _():
                sent_all(hids[h].at[pl.ds(0, n_tp - 1)], sems.hd.send.at[h])

            @pl.when(c == 0)
            def _():
                sent_all(hids[h].at[0], sems.hd.send.at[h])

        sent_all(bufs.ret.at[pl.ds(0, n_ep - 1)], sems.re.send.at[0])


def buffers(n_ep, n_tp, seqs, cols, ff):
    n_y = n_tp // 2

    def array(*shape):
        return pltpu.VMEM(shape, BF16)

    return Bufs(
        part=array(n_tp, seqs, cols),
        rs=array(n_tp, seqs, cols),
        a=array(n_ep, ROWS, cols),
        x=array(n_y, n_ep, ROWS, cols),
        p=array(n_y, n_ep, ROWS, cols),
        hid_a=array(n_tp, len(EARLY) * ROWS, ff),
        hid_b=array(n_tp, (n_ep - len(EARLY)) * ROWS, ff),
        ret=array(n_ep, ROWS, cols),
        fin=array(n_ep, ROWS, cols),
    )


def semaphores(n_ep, n_tp):
    def pair(sends, recvs):
        return Pair(pltpu.SemaphoreType.DMA((sends,)), pltpu.SemaphoreType.DMA((recvs,)))

    return Sems(
        idle=pltpu.SemaphoreType.DMA((1,)),
        rs=pair(1, 1),
        x=pair(2, len(sum(SETS, ()))),
        p=pair(1, 2),
        hy=pair(2, n_tp - 2),
        hd=pair(2, 2),
        re=pair(1, 1),
    )


def run(n_ep, n_tp, hbm):
    seqs, width = hbm.tokens.shape
    length, dim = hbm.cache_keys.shape[1:]
    owned, _, ff = hbm.gate_w.shape
    cols = width // n_tp
    hbm = hbm._replace(
        lengths=hbm.lengths.reshape(1, -1),
        attn_gain=hbm.attn_gain.reshape(1, -1),
        head_gain=hbm.head_gain.reshape(1, -1),
        ffn_gain=hbm.ffn_gain.reshape(1, -1),
        mix_lambda=hbm.mix_lambda.reshape(1, -1),
        q_first_w=hbm.q_first_w.T,
        q_second_w=hbm.q_second_w.T,
        k_first_w=hbm.k_first_w.T,
        k_second_w=hbm.k_second_w.T,
        routes=hbm.routes.T,
        route_logits=hbm.route_logits.T,
    )

    def like(x):
        return pltpu.VMEM(x.shape, x.dtype)

    vm = Held(
        tokens=like(hbm.tokens),
        lengths=like(hbm.lengths),
        cache_keys=like(hbm.cache_keys),
        cache_values=like(hbm.cache_values),
        attn_gain=like(hbm.attn_gain),
        narrow_w=pltpu.VMEM((2 * dim, width), BF16),
        value_w=like(hbm.value_w),
        mix_lambda=like(hbm.mix_lambda),
        head_gain=like(hbm.head_gain),
        out_w=like(hbm.out_w),
        ffn_gain=like(hbm.ffn_gain),
        routes=like(hbm.routes),
        route_logits=like(hbm.route_logits),
        gate_up_w=pltpu.VMEM((owned, width, 2 * ff), BF16),
        down_w=like(hbm.down_w),
    )
    work = Work(
        queries=pltpu.VMEM((seqs * dim, dim), BF16),
        scores=pltpu.VMEM((length, dim), F32),
        mixed=pltpu.VMEM((seqs, length), BF16),
        len_row=pltpu.VMEM((8, dim), jnp.int32),
        narrow=pltpu.VMEM((2 * dim, dim), F32),
    )

    def kernel(hbm, out_ref, vm, work, bufs, wide, sems, load_sems):
        loads = plan_loads(hbm, vm, load_sems)
        for group in loads:
            for copy in group:
                copy.start()
        e, t = lax.axis_index("ep"), lax.axis_index("tp")
        barrier = pltpu.get_barrier_semaphore()
        for k in range(1, n_tp):
            pl.semaphore_signal(barrier, inc=1, device_id=(e, (t + k) % n_tp), device_id_type=MESH)
        for k in range(1, n_ep):
            pl.semaphore_signal(barrier, inc=1, device_id=((e + k) % n_ep, t), device_id_type=MESH)
        attend(loads, vm, work, bufs.part)
        with scope("bar"):
            pl.semaphore_wait(barrier, n_tp + n_ep - 2)
        exchange((n_ep, n_tp, owned), loads, vm, bufs, wide, sems, out_ref)

    return pl.pallas_call(
        kernel,
        out_shape=pltpu.VMEM((seqs, cols), OUT),
        in_specs=[Args(*[pl.BlockSpec(memory_space=pl.ANY)] * len(hbm))],
        out_specs=pl.BlockSpec(memory_space=pltpu.VMEM),
        scratch_shapes=[
            vm,
            work,
            buffers(n_ep, n_tp, seqs, cols, ff),
            pltpu.VMEM((n_ep * ROWS, 128), F32),
            semaphores(n_ep, n_tp),
            pltpu.SemaphoreType.DMA((N_LOADS,)),
        ],
        compiler_params=pltpu.CompilerParams(
            vmem_limit_bytes=56 * 1024 * 1024, collective_id=0, has_side_effects=True
        ),
    )(hbm)


OUT = F32


def solution(mesh):
    n_ep, n_tp = mesh.shape["ep"], mesh.shape["tp"]

    def per_device(*args):
        return run(n_ep, n_tp, Args(*args)).astype(BF16)

    rows, heads, both = P("ep", None), P(None, "tp"), P("ep", None, "tp")
    return jax.shard_map(
        per_device,
        mesh=mesh,
        in_specs=(
            rows, P("ep"), both, both, P(), heads, heads, heads, heads, heads,
            P("tp"), P(), P("tp", None), P(), rows, rows, both, both, both,
        ),
        out_specs=P("ep", "tp"),
        check_vma=False,
    )
```

```python
import itertools
from typing import Any, NamedTuple

import jax
import jax.numpy as jnp
from jax import lax
from jax.experimental import pallas as pl
from jax.experimental.pallas import tpu as pltpu
from jax.sharding import PartitionSpec as P

EPS = 1e-06
LIMIT = 7.0
ALPHA = 1.702
MESH = pl.DeviceIdType.MESH
F32 = jnp.float32
BF16 = jnp.bfloat16
VALUE_CUTS = (0, 16, 28, 32)
KEY_CHUNKS = 4
ROWS = 16
SETS = ((0, 1, 2), (3, 4, 8)), ((5, 6, 7, 9), (10, 11, 12), (13, 14, 15))
EARLY = sum(SETS[0], ())
scope = jax.named_scope


class Args(NamedTuple):
    tokens: Any
    lengths: Any
    cache_keys: Any
    cache_values: Any
    attn_gain: Any
    q_first_w: Any
    q_second_w: Any
    k_first_w: Any
    k_second_w: Any
    value_w: Any
    mix_lambda: Any
    head_gain: Any
    out_w: Any
    ffn_gain: Any
    routes: Any
    route_logits: Any
    gate_w: Any
    up_w: Any
    down_w: Any


class Held(NamedTuple):
    tokens: Any
    lengths: Any
    cache_keys: Any
    cache_values: Any
    attn_gain: Any
    narrow_w: Any
    value_w: Any
    mix_lambda: Any
    head_gain: Any
    out_w: Any
    ffn_gain: Any
    routes: Any
    route_logits: Any
    gate_up_w: Any
    down_w: Any


class Loads(NamedTuple):
    tokens: Any
    attn_gain: Any
    narrow_w: Any
    lengths: Any
    mix_lambda: Any
    head_gain: Any
    ffn_gain: Any
    routes: Any
    route_logits: Any
    keys: Any
    value_w: Any
    values: Any
    out_w: Any
    gate_up_w: Any
    down_w: Any


class Work(NamedTuple):
    queries: Any
    scores: Any
    mixed: Any
    len_row: Any
    narrow: Any


class Bufs(NamedTuple):
    part: Any
    rs: Any
    a: Any
    x: Any
    p: Any
    hid_a: Any
    hid_b: Any
    ret: Any
    fin: Any


class Pair(NamedTuple):
    send: Any
    recv: Any


class Sems(NamedTuple):
    idle: Any
    rs: Pair
    x: Pair
    p: Pair
    hy: Pair
    hd: Pair
    re: Pair


def dot(a, b):
    return jnp.dot(a, b, preferred_element_type=F32)


def dot_nt(a, b):
    return lax.dot_general(a, b, (((1,), (1,)), ((), ())), preferred_element_type=F32)


def iota(shape, dim):
    return lax.broadcasted_iota(jnp.int32, shape, dim)


class Pieces(NamedTuple):
    copies: Any
    whole: Any

    def start(self):
        for copy in self.copies:
            copy.start()

    def wait(self):
        self.whole.wait()


def plan_loads(hbm, vm, sems):
    count = iter(range(N_LOADS))

    def copy(src, dst):
        return (pltpu.make_async_copy(src, dst, sems.at[next(count)]),)

    def pieces(whole, parts):
        sem = sems.at[next(count)]
        return Pieces([pltpu.make_async_copy(s, d, sem) for s, d in parts], pltpu.make_async_copy(whole, whole, sem))

    half = hbm.q_first_w.shape[0]
    rows = hbm.cache_keys.shape[1] // KEY_CHUNKS
    ff = hbm.gate_w.shape[2]
    narrow = (hbm.q_first_w, hbm.q_second_w, hbm.k_first_w, hbm.k_second_w)
    spans = [pl.ds(i * rows, rows) for i in range(KEY_CHUNKS)]
    blocks = [pl.ds(a, b - a) for a, b in itertools.pairwise(VALUE_CUTS)]
    return Loads(
        tokens=copy(hbm.tokens, vm.tokens),
        attn_gain=copy(hbm.attn_gain, vm.attn_gain),
        narrow_w=(
            pieces(vm.narrow_w, [(w, vm.narrow_w.at[pl.ds(i * half, half)]) for i, w in enumerate(narrow)]),
        ),
        lengths=copy(hbm.lengths, vm.lengths),
        mix_lambda=copy(hbm.mix_lambda, vm.mix_lambda),
        head_gain=copy(hbm.head_gain, vm.head_gain),
        ffn_gain=copy(hbm.ffn_gain, vm.ffn_gain),
        routes=copy(hbm.routes, vm.routes),
        route_logits=copy(hbm.route_logits, vm.route_logits),
        keys=sum((copy(hbm.cache_keys.at[:, s, :], vm.cache_keys.at[:, s, :]) for s in spans), ()),
        value_w=copy(hbm.value_w, vm.value_w),
        values=sum((copy(hbm.cache_values.at[b], vm.cache_values.at[b]) for b in blocks), ()),
        out_w=copy(hbm.out_w, vm.out_w),
        gate_up_w=(
            pieces(
                vm.gate_up_w,
                [(hbm.gate_w, vm.gate_up_w.at[:, :, pl.ds(0, ff)]), (hbm.up_w, vm.gate_up_w.at[:, :, pl.ds(ff, ff)])],
            ),
        ),
        down_w=copy(hbm.down_w, vm.down_w),
    )


N_LOADS = 12 + KEY_CHUNKS + len(VALUE_CUTS)


def wait(copies):
    for copy in copies:
        copy.wait()


def attend(loads, vm, work, part_ref):
    with scope("load"):
        wait(loads.tokens + loads.attn_gain)
    with scope("proj"):
        seqs, width = vm.tokens.shape
        length, dim = vm.cache_keys.shape[1:]
        half = dim // 2
        tok = vm.tokens[...].astype(F32)
        mean_sq = jnp.mean(tok * tok, axis=1, keepdims=True)
        normed = (tok * lax.rsqrt(mean_sq + EPS) * vm.attn_gain[...]).astype(BF16)
        wait(loads.narrow_w)
        wait(loads.lengths)
        work.len_row[...] = jnp.zeros_like(work.len_row)
        work.narrow[...] = jnp.zeros_like(work.narrow)
        narrow = dot_nt(vm.narrow_w[...], normed).astype(BF16).astype(F32)
        for i in range(4):
            lane = i % 2 * half
            work.narrow[i * half : (i + 1) * half, lane : lane + seqs] = narrow[i * half : (i + 1) * half, :]
        for lane in (0, half):
            work.len_row[0:1, lane : lane + seqs] = vm.lengths[...]
        q_t = work.narrow[0:dim, :] * (half ** (-0.5))
        k_t = work.narrow[dim : 2 * dim, :]
        owner = iota((dim, dim), 1) - jnp.where(iota((dim, dim), 0) < half, 0, half)
        for s in range(seqs):
            work.queries[s * dim : (s + 1) * dim, :] = jnp.where(owner == s, q_t, 0.0).astype(BF16)
        own = jnp.sum(q_t * k_t, axis=0, keepdims=True)
        lens = work.len_row[0:1, :]
    rows = length // KEY_CHUNKS
    top = own
    for i in range(KEY_CHUNKS):
        with scope("wk"):
            loads.keys[i].wait()
        with scope("qk"):
            got = 0.0
            for first in range(0, seqs, seqs // 1):
                mine = range(first, first + seqs // 1)
                keys = jnp.concatenate([vm.cache_keys[s, i * rows : (i + 1) * rows, :] for s in mine], axis=1)
                got = got + dot(keys, work.queries[first * dim : (first + seqs // 1) * dim, :])
            valid = iota((rows, dim), 0) + i * rows < lens
            got = jnp.where(valid, got, -jnp.inf)
            work.scores[i * rows : (i + 1) * rows, :] = got
            top = jnp.maximum(top, jnp.max(got, axis=0, keepdims=True))
    with scope("soft"):
        wait(loads.mix_lambda + loads.value_w)
        new_value = dot(normed, vm.value_w[...]).astype(BF16).astype(F32)
        own_raised = jnp.exp(own - top)
        total = own_raised
        for i in range(KEY_CHUNKS):
            raised = jnp.exp(work.scores[i * rows : (i + 1) * rows, :] - top)
            work.scores[i * rows : (i + 1) * rows, :] = raised
            total = total + jnp.sum(raised, axis=0, keepdims=True)
        share = jnp.where(iota((1, dim), 1) < half, 1.0, -vm.mix_lambda[...]) / total
        for i in range(length // dim):
            block = (work.scores[i * dim : (i + 1) * dim, :] * share).T
            mixed = block[0:seqs, :] + block[half : half + seqs, :]
            work.mixed[:, i * dim : (i + 1) * dim] = mixed.astype(BF16)
        own_w = jnp.broadcast_to(own_raised * share, (dim, dim)).T
        own_col = (own_w[0:seqs, :] + own_w[half : half + seqs, :]).astype(BF16).astype(F32)
    group = 16
    place = iota((group, dim), 0)
    outs = [jnp.zeros((group, dim), F32) for _ in range(seqs // group)]
    for i, (start, stop) in enumerate(itertools.pairwise(VALUE_CUTS)):
        with scope("wv"):
            loads.values[i].wait()
        with scope("pv"):
            for s in range(start, stop, 2):
                g = s // group
                both = jnp.concatenate([vm.cache_values[s], vm.cache_values[s + 1]], axis=1)
                got = dot(work.mixed[g * group : (g + 1) * group, :], both)
                outs[g] = outs[g] + jnp.where(place == s % group, got[:, 0:dim], 0.0)
                outs[g] = outs[g] + jnp.where(place == s % group + 1, got[:, dim : 2 * dim], 0.0)
    with scope("head"):
        wait(loads.head_gain)
        head_out = jnp.concatenate(outs, axis=0) + own_col * new_value
        mean_sq = jnp.mean(head_out * head_out, axis=1, keepdims=True)
        attended = (head_out * lax.rsqrt(mean_sq + EPS) * vm.head_gain[...]).astype(BF16)
        wait(loads.out_w)
        blocks, _, cols = part_ref.shape
        for b in range(blocks):
            part_ref[b] = dot(attended, vm.out_w[:, b * cols : (b + 1) * cols]).astype(BF16)


def remote(src, dst, send, recv, ep, tp):
    return pltpu.make_async_remote_copy(
        src_ref=src, dst_ref=dst, send_sem=send, recv_sem=recv, device_id=(ep, tp), device_id_type=MESH
    )


def slot_tables(vm, slots):
    routes, logits = vm.routes[...], vm.route_logits[...]
    top, seqs = routes.shape
    logits = jnp.exp(logits - jnp.max(logits, axis=0, keepdims=True))
    weights = logits / jnp.sum(logits, axis=0, keepdims=True)
    slot = iota((slots, seqs), 0)
    named = jnp.zeros((slots, seqs), F32)
    weight = jnp.zeros((slots, seqs), F32)
    for k in range(top):
        hit = routes[k : k + 1, :] == slot // 4
        named = jnp.where(hit, 1.0, named)
        weight = jnp.where(hit, weights[k : k + 1, :], weight)
    before = (iota((seqs, seqs), 0) < iota((seqs, seqs), 1)).astype(F32).astype(BF16)
    rank = dot(named.astype(BF16), before)
    taken = (named > 0.5) & (rank == (slot % 4).astype(F32))
    return jnp.where(taken, 1.0, 0.0).astype(BF16), jnp.where(taken, weight, 0.0)


def is_in(e, groups):
    return sum(1 // (1 + (e - g) * (e - g)) for g in groups)


def runs(groups):
    firsts = [g for g in groups if g - 1 not in groups]
    return [(g, next(n for n in itertools.count(1) if g + n not in groups)) for g in firsts]


def far_first(sizes):
    every = [()]
    for n in sizes:
        every = [o + (d,) for o in every for d in range(n)]
    hops = lambda o: sum(min(d, n - d) for d, n in zip(o, sizes, strict=True))
    return sorted(every, key=hops, reverse=True)


def exchange(sizes, loads, vm, bufs, wide, sems, out_ref):
    n_ep, n_tp, owned = sizes
    n_y, n_x = n_tp // 2, 4
    n_z = n_ep // n_x
    e, t = lax.axis_index("ep"), lax.axis_index("tp")
    y, c = t // 2, t % 2
    z, x = e // n_x, e % n_x
    partner = t + 1 - 2 * c
    seqs, cols = bufs.part.shape[1:]
    slots = n_ep * ROWS
    lanes = 128

    def ep_at(dz, dx):
        return (z + dz) % n_z * n_x + (x + dx) % n_x

    def tp_at(dy, dc):
        return (y + dy) % n_y * 2 + (c + dc + 2) % 2

    def send(src, dst, sent, got, ep, tp):
        remote(src, dst, sent, got, ep, tp).start()

    def sent_all(buf, sem):
        remote(buf, buf, sem, sems.idle.at[0], e, partner).wait_send()

    def arrive(buf, sem):
        remote(buf, buf, sems.idle.at[0], sem, e, partner).wait_recv()

    with scope("rs"):
        for dy, dc in far_first((n_y, 2)):
            if dy or dc:
                to = tp_at(dy, dc)
                send(bufs.part.at[to], bufs.rs.at[t], sems.rs.send.at[0], sems.rs.recv.at[0], e, to)
        wait(loads.routes + loads.route_logits + loads.ffn_gain)
        dispatch, combine = slot_tables(vm, slots)
        wide[...] = jnp.zeros_like(wide)
        wide[:, 0:seqs] = combine
        combine = jnp.concatenate([wide[i : i + lanes, :].T[0:seqs, :] for i in range(0, slots, lanes)], axis=1)
        combine_hi = combine.astype(BF16)
        combine_lo = (combine - combine_hi.astype(F32)).astype(BF16)
        start = pl.multiple_of(t * cols, cols)
        kept = vm.tokens[:, pl.ds(start, cols)].astype(F32)
        gain = vm.ffn_gain[:, pl.ds(start, cols)]
        bufs.rs[t] = bufs.part[t]
    with scope("rsw"):
        arrive(bufs.rs.at[pl.ds(0, n_tp - 1)], sems.rs.recv.at[0])
        for i in range(n_tp):
            kept = kept + bufs.rs[i].astype(F32)

    with scope("d1"):
        rows = dot(dispatch, (kept * gain).astype(BF16)).astype(BF16)
        bufs.a[...] = rows.reshape(bufs.a.shape)
        mine = sum(i * is_in(e, of) for i, of in enumerate(sum(SETS, ())))
        for dz, dx, dy in far_first((n_z, n_x, n_y)):
            to = ep_at(dz, dx)
            if dz or dx or dy:
                which = 1 if dy else 0
                send(bufs.a.at[to], bufs.x.at[y, e], sems.x.send.at[which], sems.x.recv.at[mine], to, tp_at(dy, 0))
        bufs.x[y, e] = bufs.a[e]

    halves = (EARLY, sum(SETS[1], ()))
    hids = (bufs.hid_a, bufs.hid_b)
    ff = vm.gate_up_w.shape[2] // 2

    def of_expert(results):
        expert = iota(results[0].shape, 0) % ROWS // 4
        total = results[0]
        for j in range(1, owned):
            total = jnp.where(expert == j, results[j], total)
        return total

    def gate_up(buf, core, groups):
        squares = jnp.zeros((len(groups) * ROWS, lanes), F32)
        tiles, begins = [], []
        for i in range(n_y):
            begin = pl.multiple_of((2 * i + core) * cols, cols)
            begins.append(begin)
            tile = jnp.concatenate([buf[i, g] for g in groups], axis=0)
            tiles.append(tile)
            tile = tile.astype(F32) * (1.0 / vm.ffn_gain[:, pl.ds(begin, cols)])
            for j in range(0, cols, lanes):
                squares = squares + tile[:, j : j + lanes] * tile[:, j : j + lanes]
        tiles = jnp.concatenate(tiles, axis=1)
        got = [
            dot(tiles, jnp.concatenate([vm.gate_up_w[j, pl.ds(b, cols), :] for b in begins], axis=0))
            for j in range(owned)
        ]
        return of_expert(got), squares

    def collect(h):
        for of in SETS[h]:
            place = sum(SETS, ()).index(of)
            copies = n_y * len(of)

            @pl.when(is_in(e, of) == 0)
            def _():
                arrive(bufs.x.at[0, pl.ds(0, copies)], sems.x.recv.at[place])

            @pl.when(is_in(e, of) == 1)
            def _():
                arrive(bufs.x.at[0, pl.ds(0, copies - 1)], sems.x.recv.at[place])

            for first, count in runs(of):
                at = pl.ds(first, count)
                send(bufs.x.at[:, at], bufs.p.at[:, at], sems.p.send.at[0], sems.p.recv.at[h], e, partner)

    for h, groups in enumerate(halves):
        if h == 0:
            with scope("xw"):
                collect(0)
            wait(loads.gate_up_w + loads.down_w)
        else:
            with scope("xb"):
                pl.when(c == 0)(lambda: collect(1))
        with scope("gu"):
            first, first_squares = gate_up(bufs.x, c, groups)
        if h == 0:
            with scope("xc"):
                pl.when(c == 1)(lambda: collect(1))
        with scope("pw"):
            arrive(bufs.p.at[:, pl.ds(0, len(groups))], sems.p.recv.at[h])
        with scope("gv"):
            both, squares = gate_up(bufs.p, 1 - c, groups)
            both, squares = both + first, squares + first_squares
            scale = lax.rsqrt(jnp.sum(squares, axis=1, keepdims=True) / (n_tp * cols) + EPS)
            both = both * scale
            gate = jnp.minimum(both[:, :ff], LIMIT)
            up = jnp.clip(both[:, ff:], -LIMIT, LIMIT)
            mine = hids[h].at[t]
            mine[...] = ((up + 1.0) * gate / (1.0 + jnp.exp(-ALPHA * gate))).astype(BF16)

            for (dy,) in far_first((n_y,)):
                if dy:
                    place = h * (n_y - 1) + dy - 1
                    send(mine, mine, sems.hy.send.at[h], sems.hy.recv.at[place], e, tp_at(dy, 1 - c))
            send(mine, mine, sems.hd.send.at[h], sems.hd.recv.at[h], e, partner)
    for h, groups in enumerate(halves):
        with scope("hyw"):

            @pl.when(c == 1)
            def _():
                for (dy,) in reversed(far_first((n_y,))):
                    if dy:
                        block = hids[h].at[pl.ds((y + dy) % n_y * 2, 2)]
                        arrive(block, sems.hy.recv.at[h * (n_y - 1) + n_y - dy - 1])
                        send(block, block, sems.hd.send.at[h], sems.hd.recv.at[h], e, partner)
                arrive(hids[h].at[0], sems.hd.recv.at[h])

            @pl.when(c == 0)
            def _():
                arrive(hids[h].at[pl.ds(0, n_tp - 1)], sems.hd.recv.at[h])

        with scope("down"):
            hidden = jnp.concatenate([hids[h][i] for i in range(n_tp)], axis=1)
            result = of_expert([dot(hidden, vm.down_w[j]) for j in range(owned)]).astype(BF16)

            for i, g in enumerate(groups):
                bufs.ret[g] = result[i * ROWS : (i + 1) * ROWS, :]
            for g in reversed(groups):

                @pl.when(e != g)
                def _():
                    send(bufs.ret.at[g], bufs.fin.at[e], sems.re.send.at[0], sems.re.recv.at[0], g, t)

                @pl.when(e == g)
                def _():
                    bufs.fin[g] = bufs.ret[g]

    with scope("rew"):
        arrive(bufs.fin.at[pl.ds(0, n_ep - 1)], sems.re.recv.at[0])
    with scope("fin"):
        back = bufs.fin[...].reshape(slots, cols)
        out_ref[...] = (kept + dot(combine_hi, back) + dot(combine_lo, back)).astype(out_ref.dtype)
        sent_all(bufs.part.at[pl.ds(0, n_tp - 1)], sems.rs.send.at[0])
        sent_all(bufs.x.at[0, pl.ds(0, n_ep - 1)], sems.x.send.at[0])
        sent_all(bufs.x.at[pl.ds(0, n_y - 1)], sems.x.send.at[1])
        sent_all(bufs.x, sems.p.send.at[0])
        for h in range(2):
            sent_all(hids[h].at[pl.ds(0, n_y - 1)], sems.hy.send.at[h])

            @pl.when(c == 1)
            def _():
                sent_all(hids[h].at[pl.ds(0, n_tp - 1)], sems.hd.send.at[h])

            @pl.when(c == 0)
            def _():
                sent_all(hids[h].at[0], sems.hd.send.at[h])

        sent_all(bufs.ret.at[pl.ds(0, n_ep - 1)], sems.re.send.at[0])


def buffers(n_ep, n_tp, seqs, cols, ff):
    n_y = n_tp // 2

    def array(*shape):
        return pltpu.VMEM(shape, BF16)

    return Bufs(
        part=array(n_tp, seqs, cols),
        rs=array(n_tp, seqs, cols),
        a=array(n_ep, ROWS, cols),
        x=array(n_y, n_ep, ROWS, cols),
        p=array(n_y, n_ep, ROWS, cols),
        hid_a=array(n_tp, len(EARLY) * ROWS, ff),
        hid_b=array(n_tp, (n_ep - len(EARLY)) * ROWS, ff),
        ret=array(n_ep, ROWS, cols),
        fin=array(n_ep, ROWS, cols),
    )


def semaphores(n_ep, n_tp):
    def pair(sends, recvs):
        return Pair(pltpu.SemaphoreType.DMA((sends,)), pltpu.SemaphoreType.DMA((recvs,)))

    return Sems(
        idle=pltpu.SemaphoreType.DMA((1,)),
        rs=pair(1, 1),
        x=pair(2, len(sum(SETS, ()))),
        p=pair(1, 2),
        hy=pair(2, n_tp - 2),
        hd=pair(2, 2),
        re=pair(1, 1),
    )


def run(n_ep, n_tp, hbm):
    seqs, width = hbm.tokens.shape
    length, dim = hbm.cache_keys.shape[1:]
    owned, _, ff = hbm.gate_w.shape
    cols = width // n_tp
    hbm = hbm._replace(
        lengths=hbm.lengths.reshape(1, -1),
        attn_gain=hbm.attn_gain.reshape(1, -1),
        head_gain=hbm.head_gain.reshape(1, -1),
        ffn_gain=hbm.ffn_gain.reshape(1, -1),
        mix_lambda=hbm.mix_lambda.reshape(1, -1),
        q_first_w=hbm.q_first_w.T,
        q_second_w=hbm.q_second_w.T,
        k_first_w=hbm.k_first_w.T,
        k_second_w=hbm.k_second_w.T,
        routes=hbm.routes.T,
        route_logits=hbm.route_logits.T,
    )

    def like(x):
        return pltpu.VMEM(x.shape, x.dtype)

    vm = Held(
        tokens=like(hbm.tokens),
        lengths=like(hbm.lengths),
        cache_keys=like(hbm.cache_keys),
        cache_values=like(hbm.cache_values),
        attn_gain=like(hbm.attn_gain),
        narrow_w=pltpu.VMEM((2 * dim, width), BF16),
        value_w=like(hbm.value_w),
        mix_lambda=like(hbm.mix_lambda),
        head_gain=like(hbm.head_gain),
        out_w=like(hbm.out_w),
        ffn_gain=like(hbm.ffn_gain),
        routes=like(hbm.routes),
        route_logits=like(hbm.route_logits),
        gate_up_w=pltpu.VMEM((owned, width, 2 * ff), BF16),
        down_w=like(hbm.down_w),
    )
    work = Work(
        queries=pltpu.VMEM((seqs * dim, dim), BF16),
        scores=pltpu.VMEM((length, dim), F32),
        mixed=pltpu.VMEM((seqs, length), BF16),
        len_row=pltpu.VMEM((8, dim), jnp.int32),
        narrow=pltpu.VMEM((2 * dim, dim), F32),
    )

    def kernel(hbm, out_ref, vm, work, bufs, wide, sems, load_sems):
        loads = plan_loads(hbm, vm, load_sems)
        for group in loads:
            for copy in group:
                copy.start()
        e, t = lax.axis_index("ep"), lax.axis_index("tp")
        barrier = pltpu.get_barrier_semaphore()
        for k in range(1, n_tp):
            pl.semaphore_signal(barrier, inc=1, device_id=(e, (t + k) % n_tp), device_id_type=MESH)
        for k in range(1, n_ep):
            pl.semaphore_signal(barrier, inc=1, device_id=((e + k) % n_ep, t), device_id_type=MESH)
        attend(loads, vm, work, bufs.part)
        with scope("bar"):
            pl.semaphore_wait(barrier, n_tp + n_ep - 2)
        exchange((n_ep, n_tp, owned), loads, vm, bufs, wide, sems, out_ref)

    return pl.pallas_call(
        kernel,
        out_shape=pltpu.VMEM((seqs, cols), OUT),
        in_specs=[Args(*[pl.BlockSpec(memory_space=pl.ANY)] * len(hbm))],
        out_specs=pl.BlockSpec(memory_space=pltpu.VMEM),
        scratch_shapes=[
            vm,
            work,
            buffers(n_ep, n_tp, seqs, cols, ff),
            pltpu.VMEM((n_ep * ROWS, 128), F32),
            semaphores(n_ep, n_tp),
            pltpu.SemaphoreType.DMA((N_LOADS,)),
        ],
        compiler_params=pltpu.CompilerParams(
            vmem_limit_bytes=56 * 1024 * 1024, collective_id=0, has_side_effects=True
        ),
    )(hbm)


OUT = F32


def solution(mesh):
    n_ep, n_tp = mesh.shape["ep"], mesh.shape["tp"]

    def per_device(*args):
        return run(n_ep, n_tp, Args(*args)).astype(BF16)

    rows, heads, both = P("ep", None), P(None, "tp"), P("ep", None, "tp")
    return jax.shard_map(
        per_device,
        mesh=mesh,
        in_specs=(
            rows, P("ep"), both, both, P(), heads, heads, heads, heads, heads,
            P("tp"), P(), P("tp", None), P(), rows, rows, both, both, both,
        ),
        out_specs=P("ep", "tp"),
        check_vma=False,
    )
```
